32 devices in a mesh: ep: 8 (over z, y), tp: 4 (over x, core).
Axes of the slice: x: 2, y: 2, z: 4, core: 2. Of those that a mesh axis runs over, the one named last changes fastest.
Arguments:
- tokens: bfloat16 [128, 1024], P('ep', 'tp'), may hold values from -75 to 75
- gain_mix: float32 [1024], replicated, may hold values from 0.1 to 1.9
- w_query: bfloat16 [1024, 512], P(None, 'tp'), may hold values from -0.1875 to 0.1875
- w_key: bfloat16 [1024, 512], P(None, 'tp'), may hold values from -0.1875 to 0.1875
- w_value: bfloat16 [1024, 512], P(None, 'tp'), may hold values from -0.1875 to 0.1875
- w_outgate: bfloat16 [1024, 512], P(None, 'tp'), may hold values from -0.1875 to 0.1875
- w_input_gate: bfloat16 [1024, 4], P(None, 'tp'), may hold values from -0.1875 to 0.1875
- w_forget_gate: bfloat16 [1024, 4], P(None, 'tp'), may hold values from -0.1875 to 0.1875
- w_mix_out: bfloat16 [512, 1024], P(None, 'tp'), may hold values from -0.25 to 0.25
- cell_state: float32 [128, 4, 128, 128], P('ep', 'tp'), may hold values from -3 to 3
- norm_state: float32 [128, 4, 128], P('ep', 'tp'), may hold values from -3 to 3
- max_state: float32 [128, 4], P('ep', 'tp'), may hold values from -2 to 143
- gain_ffn: float32 [1024], replicated, may hold values from 0.1 to 1.9
- route_ids: int32 [128, 2], P('ep'), may hold values from 0 to 7, all different within a row; in each aligned block of 16 rows (0 to 15, 16 to 31, ...) at most 8 rows name the same one
- route_logits: float32 [128, 2], P('ep'), may hold values from -5 to 5
- expert_gate: bfloat16 [8, 1024, 1408], P('ep', None, 'tp'), may hold values from -0.1875 to 0.1875
- expert_up: bfloat16 [8, 1024, 1408], P('ep', None, 'tp'), may hold values from -0.1875 to 0.1875
- expert_down: bfloat16 [8, 1408, 1024], P('ep', 'tp'), may hold values from -0.15625 to 0.15625
- dense_gate: bfloat16 [1024, 3072], P('tp', 'ep'), may hold values from -0.1875 to 0.1875
- dense_up: bfloat16 [1024, 3072], P('tp', 'ep'), may hold values from -0.1875 to 0.1875
- dense_down: bfloat16 [3072, 1024], P('ep', 'tp'), may hold values from -0.3125 to 0.3125
- dense_mix: bfloat16 [1024], P('tp'), may hold values from -0.1875 to 0.1875
Outputs:
- layer_out: bfloat16 [128, 1024], P('ep', 'tp')
The draws below stay inside these ranges and needn't reach their ends.
Inputs may be any that keep to these rules, and one draw needn't show every extreme that they name: `route_ids`: each row names 2 different experts. Among the 16 tokens of one index of ep no expert is named more than 8 times, and in every draw some expert is named exactly 8 times by the tokens of one index of ep.
All inputs are finite; a program needn't handle non-finite values.
Results may differ from the reference program's by a relative error of at most 0.013.
Values may be sent and summed in bfloat16 or wider, within the bound.
A program may use at most 64 MiB of HBM per device.

```python
import math
import jax
import jax.numpy as jnp
import numpy as np
from jax import lax

D = 1024
HEADS = 4
HEAD = 128
FF_EXP = 1408
DENSE_FF = 3072
SEQ_DEV = 16
TOP = 2
CAP = 8
WIDTH = 512
BATCH = 128
EXPERTS = 8
N_TP = 4


def draw_tokens(key, part):
    key_base, key_group, key_block = jax.random.split(key, 3)
    base = jnp.clip(jax.random.normal(key_base, (BATCH, D), jnp.float32), -5.0, 5.0)
    group_scale = jnp.exp(jax.random.uniform(key_group, (D // 16,), jnp.float32, -1.1, 1.1))
    block_scale = jnp.exp(jax.random.uniform(key_block, (4,), jnp.float32, -1.1, 1.1))
    columns = jnp.arange(D)
    values = base * group_scale[columns // 16][None, :] * block_scale[columns // (D // 4)][None, :]
    return values.astype(jnp.bfloat16)


def draw_max_state(key, part):
    key_base = jax.random.fold_in(key, 0)
    base = jax.random.uniform(key_base, (BATCH, HEADS), jnp.float32, -2.0, 3.0)
    return base


def shard_levels(stream_key, dims, cuts, low, top_value):
    level, own = 1.0, jax.random.fold_in(stream_key, 6)
    for position, parts in cuts:
        heights = jnp.exp(jax.random.uniform(jax.random.fold_in(own, position), (parts,), jnp.float32, low / len(cuts), top_value / len(cuts)))
        level = level * jnp.repeat(heights, dims[position] // parts).reshape([-1 if axis == position else 1 for axis in range(len(dims))])
    return level


def deal_out(stream_key, own, number, rows, amount, top, limit, skew):
    sequence = jax.random.permutation(stream_key, amount)
    heavy_load, ordinary = load_shares(amount, rows * top, limit, skew, True), load_shares(amount, rows * top, limit, skew, False)
    places = jnp.arange(amount)

    def named(tallies, rotation):
        used = int((tallies > 0).sum())
        fixed = max(1, used // 4)
        passed = fixed + (places - fixed + rotation * (used - fixed)) % max(1, amount - fixed)
        return jnp.zeros((amount,), jnp.int32).at[sequence[jnp.where(places < fixed, places, passed)]].set(jnp.asarray(tallies, jnp.int32))

    tallies = jnp.where(number % 4 == 0, named(heavy_load, number // 4), named(ordinary, number - number // 4 - 1))
    mixed = jax.random.permutation(jax.random.fold_in(own, 3), amount)
    giver, sink = mixed[0:amount // 2 * 2:2], mixed[1:amount // 2 * 2:2]
    room = jnp.minimum(tallies[giver] - 1, limit - tallies[sink]) // 2
    room = jnp.where((giver == sequence[0]) | (sink == sequence[0]) | (tallies[sink] == 0), 0, jnp.maximum(room, 0))
    passed = jax.random.randint(jax.random.fold_in(own, 4), (amount // 2,), 0, 1 << 20) % (room + 1)
    tallies = tallies.at[giver].add(-passed).at[sink].add(passed)
    members = jnp.searchsorted(jnp.cumsum(tallies), jnp.arange(rows * top), side="right").astype(jnp.int32)
    table = members.reshape(top, rows).T
    table = table[jax.random.permutation(jax.random.fold_in(own, 1), rows)]
    rotation = jax.random.randint(jax.random.fold_in(own, 2), (rows, 1), 0, top)
    return jnp.take_along_axis(table, (jnp.arange(top)[None, :] + rotation) % top, axis=1)


def load_shares(count, total, most, skew, full):
    weights = [(1 << 20) // math.isqrt(standing ** skew) + 1 for standing in range(1, count + 1)]
    largest = most if full else min(most, max(-(-total // count), total * weights[0] // sum(weights)))
    least = 1 if total - largest >= count - 1 else 0
    counts, spare = [largest] + [least] * (count - 1), total - largest - least * (count - 1)
    while spare > 0:
        free = [i for i in range(1, count) if counts[i] < largest] or [i for i in range(1, count) if counts[i] < most]
        mass, budget = sum([weights[i] for i in free]), spare
        for i in free:
            more = min(most - counts[i], max(1, budget * weights[i] // mass), spare)
            counts[i] = counts[i] + more
            spare = spare - more
    return np.array(counts)


def normal_values(key, dims, scale, bound, shards=(), held_as=jnp.bfloat16):
    factor_of = shard_levels(key, dims, shards, -0.22, 0.18) if shards else 1.0
    drawn = jax.random.normal(key, dims, jnp.float32) * scale * factor_of
    return jnp.minimum(jnp.maximum(drawn, -bound), bound).astype(held_as)


def setup_inputs(seed: int = 0) -> dict:
    key_of = jax.random.split(jax.random.key(seed), 23)
    tokens = draw_tokens(jax.random.fold_in(key_of[22], 71), 0)
    gain_mix = jnp.clip(1.0 + 0.18 * jax.random.normal(key_of[1], (D,), jnp.float32), 0.1, 1.9)
    w_query = normal_values(key_of[2], (D, WIDTH), D ** -0.5, 0.1875, ((1, 4),))
    w_key = normal_values(key_of[3], (D, WIDTH), D ** -0.5, 0.1875, ((1, 4),))
    w_value = normal_values(key_of[4], (D, WIDTH), D ** -0.5, 0.1875, ((1, 4),))
    w_outgate = normal_values(key_of[5], (D, WIDTH), D ** -0.5, 0.1875, ((1, 4),))
    w_input_gate = normal_values(key_of[6], (D, HEADS), D ** -0.5, 0.1875, ((1, 4),))
    w_forget_gate = normal_values(key_of[7], (D, HEADS), D ** -0.5, 0.1875, ((1, 4),))
    w_mix_out = normal_values(key_of[8], (WIDTH, D), WIDTH ** -0.5, 0.25, ((1, 4),))
    cell_state = normal_values(key_of[9], (BATCH, HEADS, HEAD, HEAD), 0.5, 3.0, ((0, 8), (1, 4)), jnp.float32)
    norm_state = normal_values(key_of[10], (BATCH, HEADS, HEAD), 0.5, 3.0, ((0, 8), (1, 4)), jnp.float32)
    max_state = draw_max_state(jax.random.fold_in(key_of[22], 71), 0)
    gain_ffn = jnp.clip(1.0 + 0.18 * jax.random.normal(key_of[12], (D,), jnp.float32), 0.1, 1.9)
    route_ids_keys = jax.random.split(jax.random.fold_in(key_of[13], 1), BATCH // SEQ_DEV)
    route_ids_turns = jax.random.permutation(jax.random.fold_in(key_of[13], 3), BATCH // SEQ_DEV)
    route_ids = jax.vmap(lambda own, number: deal_out(jax.random.fold_in(key_of[13], 2), own, number, SEQ_DEV, EXPERTS, TOP, CAP, 2))(route_ids_keys, route_ids_turns).reshape((BATCH, TOP))
    route_logits = normal_values(key_of[14], (BATCH, TOP), 1.0, 5.0, ((0, 8),), jnp.float32)
    expert_gate = normal_values(key_of[15], (EXPERTS, D, FF_EXP), D ** -0.5, 0.1875, ((0, 8), (2, 4)))
    expert_up = normal_values(key_of[16], (EXPERTS, D, FF_EXP), D ** -0.5, 0.1875, ((0, 8), (2, 4)))
    expert_down = normal_values(key_of[17], (EXPERTS, FF_EXP, D), FF_EXP ** -0.5, 0.15625, ((0, 8), (1, 4)))
    dense_gate = normal_values(key_of[18], (D, DENSE_FF), D ** -0.5, 0.1875, ((0, 4), (1, 8)))
    dense_up = normal_values(key_of[19], (D, DENSE_FF), D ** -0.5, 0.1875, ((0, 4), (1, 8)))
    dense_down = normal_values(key_of[20], (DENSE_FF, D), (DENSE_FF // 8) ** -0.5, 0.3125, ((0, 8), (1, 4)))
    dense_mix = normal_values(key_of[21], (D,), D ** -0.5, 0.1875, ((0, 4),))
    return dict(tokens=tokens, gain_mix=gain_mix, w_query=w_query, w_key=w_key, w_value=w_value, w_outgate=w_outgate, w_input_gate=w_input_gate, w_forget_gate=w_forget_gate, w_mix_out=w_mix_out, cell_state=cell_state, norm_state=norm_state, max_state=max_state, gain_ffn=gain_ffn, route_ids=route_ids, route_logits=route_logits, expert_gate=expert_gate, expert_up=expert_up, expert_down=expert_down, dense_gate=dense_gate, dense_up=dense_up, dense_down=dense_down, dense_mix=dense_mix)


epsilon = 1e-06
highest = lax.Precision.HIGHEST

def rms_norm(rows, gain):
    values = rows.astype(jnp.float32)
    scale = lax.rsqrt(lax.optimization_barrier(jnp.mean(values * values, axis=-1, keepdims=True)) + epsilon)
    return (values * scale * gain).astype(jnp.bfloat16)

def reference(tokens, gain_mix, w_query, w_key, w_value, w_outgate, w_input_gate, w_forget_gate, w_mix_out, cell_state, norm_state, max_state, gain_ffn, route_ids, route_logits, expert_gate, expert_up, expert_down, dense_gate, dense_up, dense_down, dense_mix):
    normed_mix = rms_norm(tokens, gain_mix)

    def project(weight):
        return jnp.dot(normed_mix, weight, preferred_element_type=jnp.float32)
    query_rows = project(w_query).reshape(BATCH, HEADS, HEAD)
    key_rows = project(w_key).reshape(BATCH, HEADS, HEAD) * HEAD ** (-0.5)
    value_rows = project(w_value).reshape(BATCH, HEADS, HEAD)
    out_gate = project(w_outgate)
    input_gate = project(w_input_gate)
    carried = jax.nn.log_sigmoid(project(w_forget_gate)) + max_state
    stabilizer = jnp.maximum(carried, input_gate)
    weight_old = jnp.exp(carried - stabilizer)
    weight_new = jnp.exp(input_gate - stabilizer) * lax.optimization_barrier(jnp.sum(query_rows * key_rows, axis=-1))
    cell_read = jnp.einsum('bhd,bhde->bhe', query_rows, cell_state, precision=highest)
    numerator = weight_old[..., None] * cell_read + weight_new[..., None] * value_rows
    denominator = weight_old * lax.optimization_barrier(jnp.sum(query_rows * norm_state, axis=-1)) + weight_new
    cell_out = numerator / jnp.maximum(jnp.abs(denominator), 1.0)[..., None]
    mixed = (jax.nn.sigmoid(out_gate) * cell_out.reshape(BATCH, WIDTH)).astype(jnp.bfloat16)
    resid = (tokens.astype(jnp.float32) + jnp.dot(mixed, w_mix_out, preferred_element_type=jnp.float32)).astype(jnp.bfloat16)
    normed_ffn = rms_norm(resid, gain_ffn)
    route_weight = jax.nn.sigmoid(route_logits - route_logits[:, ::-1])
    token_rows = jnp.repeat(normed_ffn, TOP, axis=0)
    flat_ids = route_ids.reshape(-1).astype(jnp.int32)

    def apply_expert(assignment):
        token_row, expert_id = assignment
        gate_rows = jnp.dot(token_row, expert_gate[expert_id], preferred_element_type=jnp.float32)
        up_rows = jnp.dot(token_row, expert_up[expert_id], preferred_element_type=jnp.float32)
        hidden = (jax.nn.silu(gate_rows) * up_rows).astype(jnp.bfloat16).reshape(N_TP, FF_EXP // N_TP)
        down_rows = expert_down[expert_id].reshape(N_TP, FF_EXP // N_TP, D).astype(jnp.float32)
        blocks = jnp.einsum('jf,jfd->jd', hidden.astype(jnp.float32), down_rows, precision=highest)
        blocks = lax.optimization_barrier(blocks.astype(jnp.bfloat16))
        return lax.optimization_barrier(jnp.sum(blocks.astype(jnp.float32), axis=0)).astype(jnp.bfloat16)
    expert_result = lax.map(apply_expert, (token_rows, flat_ids)).reshape(BATCH, TOP, D)
    moe = lax.optimization_barrier(jnp.sum(route_weight[..., None] * expert_result.astype(jnp.float32), axis=1))
    dense_g = jnp.dot(normed_ffn, dense_gate, preferred_element_type=jnp.float32)
    dense_u = jnp.dot(normed_ffn, dense_up, preferred_element_type=jnp.float32)
    dense_hidden = (jax.nn.silu(dense_g) * dense_u).astype(jnp.bfloat16)
    dense_out = jnp.dot(dense_hidden, dense_down, preferred_element_type=jnp.float32)
    mix_gate = jax.nn.sigmoid(jnp.dot(normed_ffn, dense_mix, preferred_element_type=jnp.float32))
    total = resid.astype(jnp.float32) + moe + mix_gate[:, None] * dense_out
    return total.astype(jnp.bfloat16)
```

```python
import functools

import jax
import jax.numpy as jnp
from jax import lax
from jax.experimental import pallas as pl
from jax.experimental.pallas import tpu as pltpu
from jax.sharding import PartitionSpec as P

F32 = jnp.float32
BF16 = jnp.bfloat16
MESH = pl.DeviceIdType.MESH
EPS = 1e-06


def dot(a, b):
    return jnp.dot(a, b, preferred_element_type=F32)


def dot_t(a, b):
    return lax.dot_general(a, b, (((1,), (1,)), ((), ())), preferred_element_type=F32)


def column(row):
    n = row.shape[1]
    square = (n, n)
    eye = lax.broadcasted_iota(jnp.int32, square, 0) == lax.broadcasted_iota(jnp.int32, square, 1)
    return jnp.sum(jnp.where(eye, jnp.broadcast_to(row, square), 0.0), axis=1, keepdims=True)


def kernel(
    n_ep,
    n_tp,
    tokens,
    gain_mix,
    w_ig,
    w_fg,
    norm_state,
    max_state,
    gain_ffn,
    ids,
    logits,
    dense_mix,
    w_q,
    w_k,
    w_v,
    w_o,
    w_mix,
    cell,
    e_gate,
    e_up,
    e_down,
    d_gate,
    d_up,
    d_down,
    out,
    tok,
    gm,
    ig_w,
    fg_w,
    ns,
    ms,
    gf,
    id_v,
    lg,
    dmx,
    wp,
    wm,
    cs,
    egu,
    ed,
    dg,
    du,
    dd,
    tok_all,
    mix_all,
    mix_own,
    dm_own,
    dm_all,
    rw_own,
    rw_all,
    res_own,
    res_all,
    read,
    give,
    take,
    c_out,
    c_in,
    local_sem,
    send_sem,
    recv_sem,
    bulk_send,
    bulk_recv,
    word_sem,
):
    i = lax.axis_index("ep")
    j = lax.axis_index("tp")
    seq, quarter = tok.shape
    head = cs.shape[-1]
    ff = e_gate.shape[1]
    lead = ff // 256 * 256
    tail = -(-(ff - lead) // 128) * 128
    half = n_tp // 2
    n_half = n_ep * half
    rows_all = n_ep * seq
    core = lax.rem(j, 2)
    other = 1 - core
    mine = i * half + j // 2
    near = j + 1 - 2 * core
    far = lax.rem(j + 2, n_tp)
    peers = [(i, lax.rem(j + step, n_tp)) for step in range(1, n_tp)]

    barrier = pltpu.get_barrier_semaphore()
    turns = [lax.rem(i + step, n_ep) for step in (n_ep // 4, n_ep - n_ep // 4)]
    bits = [1 << k for k in reversed(range(n_ep.bit_length() - 3))]
    flips = [i + b - 2 * b * lax.rem(i // b, 2) for b in bits]
    rounds = [[(t, j) for t in turns]] + [[(f, j)] for f in flips] + [peers]
    hello = peers + [p for r in rounds[:-1] for p in r]
    for peer in hello:
        pl.semaphore_signal(barrier, inc=1, device_id=peer, device_id_type=MESH)

    def tell(k):
        for peer in rounds[k]:
            pl.semaphore_signal(word_sem.at[k], inc=1, device_id=peer, device_id_type=MESH)

    def hear(k):
        pl.semaphore_wait(word_sem.at[k], len(rounds[k]))

    local = []

    def fetch(src, dst):
        copy = pltpu.make_async_copy(src, dst, local_sem.at[len(local)])
        copy.start()
        local.append(copy)
        return copy

    got_tok = fetch(tokens, tok)
    got_route = [fetch(ids, id_v), fetch(logits, lg), fetch(dense_mix, dmx)]
    got_norm = [fetch(gain_mix, gm), fetch(w_ig, ig_w), fetch(w_fg, fg_w)]
    got_proj = [
        fetch(w, wp.at[:, pl.ds(k * head, head)]) for k, w in enumerate((w_q, w_k, w_v, w_o))
    ]
    got_cell = [fetch(cell, cs), fetch(norm_state, ns), fetch(max_state, ms)]
    got_mix = fetch(w_mix, wm)
    got_gf = fetch(gain_ffn, gf)
    got_e = []
    for w, first, last in ((e_gate, 0, 2 * lead), (e_up, lead, 2 * lead + tail)):
        if lead:
            got_e.append(fetch(w.at[0, pl.ds(0, lead)], egu.at[pl.ds(first, lead)]))
        if ff > lead:
            rest = ff - lead
            got_e.append(fetch(w.at[0, pl.ds(lead, rest)], egu.at[pl.ds(last, rest)]))
    got_ed = fetch(e_down.at[0], ed)
    got_dg = fetch(d_gate, dg.at[j])
    got_du = fetch(d_up, du.at[j])

    def to_tp(src, dst, phase):
        for peer in peers:
            pltpu.make_async_remote_copy(
                src_ref=src,
                dst_ref=dst.at[j],
                send_sem=send_sem.at[phase],
                recv_sem=recv_sem.at[phase],
                device_id=peer,
                device_id_type=MESH,
            ).start()

    def wait_bytes(buf, count, sem):
        view = buf.at[pl.ds(0, count)]
        pltpu.make_async_copy(view, view, sem).wait()

    def bulk(src, dst, peer, k):
        return pltpu.make_async_remote_copy(
            src_ref=src,
            dst_ref=dst,
            send_sem=bulk_send.at[k],
            recv_sem=bulk_recv.at[k],
            device_id=(i, peer),
            device_id_type=MESH,
        )

    gate_far = bulk(d_gate, dg.at[j], far, 0)
    gate_near = bulk(d_gate, dg.at[j], near, 1)
    gate_on = bulk(dg.at[far], dg.at[far], near, 2)
    up_far = bulk(d_up, du.at[j], far, 3)
    up_near = bulk(d_up, du.at[j], near, 4)
    up_on = bulk(du.at[far], du.at[far], near, 5)
    give_on = bulk(give, take, near, 6)
    res_on = bulk(res_all.at[other], res_all.at[other], near, 7)
    down_near = bulk(d_down, dd, near, 8)

    got_tok.wait()
    pl.semaphore_wait(barrier, len(hello))
    to_tp(tok, tok_all, 0)
    tell(0)
    gate_near.start()
    up_near.start()
    down_near.start()
    gate_far.start()
    tok_all[j] = tok[...]
    for copy in got_route:
        copy.wait()
    l0, l1 = lg[0:1, :], lg[1:2, :]
    s0, s1 = jax.nn.sigmoid(l0 - l1), jax.nn.sigmoid(l1 - l0)

    def put_rw(e, carry):
        rw_own[e, :, 0:seq] = jnp.where(id_v[0:1, :] == e, s0, 0.0) + jnp.where(
            id_v[1:2, :] == e, s1, 0.0
        )
        return carry

    rw_own[...] = jnp.zeros_like(rw_own)
    lax.fori_loop(0, n_ep, put_rw, 0, unroll=8)
    rw_all[i] = rw_own[i]
    mix_row = dmx[...].astype(F32)
    mix_row = jnp.concatenate([mix_row[k : k + 1] for k in range(mix_row.shape[0])], axis=1)
    dm_own[...] = mix_row
    dm_all[j] = mix_row
    if tail > ff - lead > 0:
        for first in (2 * lead, 2 * lead + tail):
            blank = pl.ds(first + ff - lead, tail - ff + lead)
            egu[blank, :] = jnp.zeros((tail - ff + lead, egu.shape[1]), egu.dtype)
    for k in range(len(rounds) - 1):
        hear(k)
        tell(k + 1)
    to_tp(dm_own, dm_all, 2)

    def send_rw(step, carry):
        e = lax.rem(i + step, n_ep)
        pltpu.make_async_remote_copy(
            src_ref=rw_own.at[e],
            dst_ref=rw_all.at[i],
            send_sem=send_sem.at[1],
            recv_sem=recv_sem.at[1],
            device_id=(e, j),
            device_id_type=MESH,
        ).start()
        return carry

    lax.fori_loop(1, n_ep, send_rw, 0)

    for copy in got_norm:
        copy.wait()
    wait_bytes(tok_all, n_tp - 1, recv_sem.at[0])
    full = jnp.concatenate([tok_all[k] for k in range(n_tp)], axis=1).astype(F32)
    scale = lax.rsqrt(jnp.mean(full * full, axis=-1, keepdims=True) + EPS)
    normed = (full * scale * gm[...]).astype(BF16)
    normed_f = normed.astype(F32)
    ig = jnp.sum(normed_f * ig_w[...].astype(F32), axis=-1, keepdims=True)
    fg = jnp.sum(normed_f * fg_w[...].astype(F32), axis=-1, keepdims=True)
    for copy in got_proj:
        copy.wait()
    proj = dot(normed, wp[...])
    query = proj[:, :head]
    key = proj[:, head : 2 * head] * head ** (-0.5)
    value = proj[:, 2 * head : 3 * head]
    out_gate = proj[:, 3 * head :]
    for copy in got_cell:
        copy.wait()
    carried = jnp.minimum(fg, 0.0) - jnp.log1p(jnp.exp(-jnp.abs(fg))) + column(ms[...])
    stab = jnp.maximum(carried, ig)
    w_old = jnp.exp(carried - stab)
    w_new = jnp.exp(ig - stab) * jnp.sum(query * key, axis=-1, keepdims=True)
    query_t = query.T
    for b in range(seq):
        read[b : b + 1, :] = jnp.sum(query_t[:, b : b + 1] * cs[b], axis=0, keepdims=True)
    numer = w_old * read[...] + w_new * value
    denom = w_old * jnp.sum(query * ns[...], axis=-1, keepdims=True) + w_new
    cell_out = numer / jnp.maximum(jnp.abs(denom), 1.0)
    mixed = (jax.nn.sigmoid(out_gate) * cell_out).astype(BF16)
    mix_own[...] = mixed
    mix_all[j] = mixed
    to_tp(mix_own, mix_all, 3)
    up_far.start()
    hear(len(rounds) - 1)
    got_mix.wait()
    wait_bytes(mix_all, n_tp - 1, recv_sem.at[3])
    heads = jnp.concatenate([mix_all[k] for k in range(n_tp)], axis=1)
    resid = (tok[...].astype(F32) + dot(heads, wm[...])).astype(BF16)
    res_own[...] = resid

    ring = n_ep // 2

    def across(send):
        def body(t, carry):
            turn = (t + 1) // 2
            turn = lax.rem(ring // 2 + ring + jnp.where(lax.rem(t, 2) == 0, turn, -turn), ring)
            high = lax.rem(i // 2 + turn, ring)
            for low in (1, 0):
                row = 2 * high + lax.rem(i + low, 2)
                for step in reversed(range(half)):
                    send(row, lax.rem(j // 2 + step, half))
            return carry

        lax.fori_loop(0, ring, body, 0, unroll=ring <= 4)

    def send_res(row, col):
        pltpu.make_async_remote_copy(
            src_ref=res_own,
            dst_ref=res_all.at[core, mine],
            send_sem=send_sem.at[4],
            recv_sem=recv_sem.at[4],
            device_id=(row, 2 * col + other),
            device_id_type=MESH,
        ).start()
    across(send_res)
    gate_far.wait_recv()
    gate_on.start()
    wait_bytes(rw_all, n_ep - 1, recv_sem.at[1])
    wide = (n_ep, seq, rw_all.shape[-1])
    diag = lax.broadcasted_iota(jnp.int32, wide, 1) == lax.broadcasted_iota(jnp.int32, wide, 2)
    weight = jnp.where(diag, jnp.broadcast_to(rw_all[...], wide), 0.0)
    weight = jnp.sum(weight.reshape(rows_all, -1), axis=-1, keepdims=True)
    wait_bytes(dm_all, n_tp - 1, recv_sem.at[2])
    up_far.wait_recv()
    up_on.start()
    got_gf.wait()
    for copy in got_e:
        copy.wait()
    got_dg.wait()
    got_du.wait()
    gate_near.wait_recv()
    up_near.wait_recv()
    wait_bytes(res_all.at[other], n_half, recv_sem.at[4])
    res_on.start()

    def columns(part, k):
        return pl.ds(pl.multiple_of((2 * k + part) * quarter, quarter), quarter)

    def normalized(part):
        rows = res_all[part].reshape(n_ep, half, seq, quarter)
        cut, square, logit = [], 0.0, 0.0
        for k in range(half):
            block = rows[:, k].reshape(rows_all, quarter).astype(F32)
            square += jnp.sum(block * block, axis=-1, keepdims=True)
            block = (block * gf[:, columns(part, k)]).astype(BF16)
            logit += jnp.sum(block.astype(F32) * dm_all[2 * k + part], axis=-1, keepdims=True)
            cut.append(block)
        return cut, square, logit

    def expert_in(cut, part):
        return sum(dot_t(cut[k], egu[:, columns(part, k)]) for k in range(half))

    def dense_in(cut, part, w):
        return sum(dot(cut[k], w[2 * k + part]) for k in range(half))

    cut_a, square_a, logit_a = normalized(other)
    expert_a = expert_in(cut_a, other)
    gate_on.wait_recv()
    up_on.wait_recv()
    gate_a = dense_in(cut_a, other, dg)
    up_a = dense_in(cut_a, other, du)
    res_on.wait_recv()
    cut_b, square_b, logit_b = normalized(core)
    scale = lax.rsqrt((square_a + square_b) / (n_tp * quarter) + EPS)
    mix_gate = jax.nn.sigmoid((logit_a + logit_b) * scale)
    mids = (expert_a + expert_in(cut_b, core)) * scale

    def activated(g, u):
        return (g * jax.nn.sigmoid(g) * u).astype(BF16)

    rest = ff - lead
    hidden = []
    if lead:
        hidden.append(activated(mids[:, :lead], mids[:, lead : 2 * lead]))
    if rest:
        low = 2 * lead
        hidden.append(activated(mids[:, low : low + rest], mids[:, low + tail : low + tail + rest]))
    hidden = jnp.concatenate(hidden, axis=1)
    got_ed.wait()
    def expert_part(part, k):
        return dot(hidden, ed[:, columns(part, k)]) * weight

    for k in range(half):
        give[k] = expert_part(core, k).astype(BF16).reshape(n_ep, seq, quarter)
    give_on.start()
    kept = [expert_part(other, k) for k in range(half)]
    g = (gate_a + dense_in(cut_b, core, dg)) * scale
    u = (up_a + dense_in(cut_b, core, du)) * scale
    hidden = activated(g, u)
    down_near.wait_recv()
    dense = dot(hidden, dd[...]) * mix_gate
    give_on.wait_recv()
    for k in range(half):
        total = kept[k] + jnp.where(j // 2 == k, dense, 0.0)
        total += take[k].reshape(rows_all, quarter).astype(F32)
        c_out[k] = total.astype(BF16).reshape(n_ep, seq, quarter)

    def send_back(row, col):
        pltpu.make_async_remote_copy(
            src_ref=c_out.at[col, row],
            dst_ref=c_in.at[mine],
            send_sem=send_sem.at[5],
            recv_sem=recv_sem.at[5],
            device_id=(row, 2 * col + other),
            device_id_type=MESH,
        ).start()
    across(send_back)
    wait_bytes(tok_all, n_tp - 1, send_sem.at[0])
    wait_bytes(rw_all, n_ep - 1, send_sem.at[1])
    wait_bytes(dm_all, n_tp - 1, send_sem.at[2])
    wait_bytes(mix_all, n_tp - 1, send_sem.at[3])
    wait_bytes(res_all.at[other], n_half, send_sem.at[4])
    for copy in (gate_far, gate_near, gate_on, up_far, up_near, up_on, give_on, res_on, down_near):
        copy.wait_send()
    wait_bytes(c_in, n_half, send_sem.at[5])
    wait_bytes(c_in, n_half, recv_sem.at[5])
    def add(k, total):
        return total + c_in[k].astype(F32)

    total = lax.fori_loop(0, n_half, add, res_own[...].astype(F32), unroll=8)
    out[...] = total.astype(BF16)


def local(
    n_ep,
    n_tp,
    tokens,
    gain_mix,
    w_query,
    w_key,
    w_value,
    w_outgate,
    w_input_gate,
    w_forget_gate,
    w_mix_out,
    cell_state,
    norm_state,
    max_state,
    gain_ffn,
    route_ids,
    route_logits,
    expert_gate,
    expert_up,
    expert_down,
    dense_gate,
    dense_up,
    dense_down,
    dense_mix,
):
    seq, quarter = tokens.shape
    features, head = w_query.shape
    n_all = n_ep * n_tp
    ff = expert_gate.shape[2]
    dff = dense_gate.shape[1]
    vmem = pl.BlockSpec(memory_space=pltpu.VMEM)
    tail = -(-(ff % 256) // 128) * 128
    wide = 2 * (ff // 256 * 256 + tail)
    any_space = pl.BlockSpec(memory_space=pl.ANY)
    small = (
        tokens,
        gain_mix.reshape(1, -1),
        w_input_gate.reshape(1, -1),
        w_forget_gate.reshape(1, -1),
        norm_state.reshape(seq, head),
        max_state.T,
        gain_ffn.reshape(1, -1),
        route_ids.T,
        route_logits.T,
        dense_mix.reshape(-1, 128),
    )
    large = (
        w_query,
        w_key,
        w_value,
        w_outgate,
        w_mix_out,
        cell_state.reshape(seq, head, head),
        jnp.swapaxes(expert_gate, 1, 2),
        jnp.swapaxes(expert_up, 1, 2),
        expert_down,
        dense_gate,
        dense_up,
        dense_down,
    )
    return pl.pallas_call(
        functools.partial(kernel, n_ep, n_tp),
        out_shape=pltpu.VMEM((seq, quarter), BF16),
        in_specs=[any_space] * (len(small) + len(large)),
        out_specs=vmem,
        scratch_shapes=[pltpu.VMEM(x.shape, x.dtype) for x in small]
        + [
            pltpu.VMEM((features, 4 * head), BF16),
            pltpu.VMEM(w_mix_out.shape, BF16),
            pltpu.VMEM((seq, head, head), F32),
            pltpu.VMEM((wide, features), BF16),
            pltpu.VMEM((ff, features), BF16),
            pltpu.VMEM((n_tp, quarter, dff), BF16),
            pltpu.VMEM((n_tp, quarter, dff), BF16),
            pltpu.VMEM(dense_down.shape, BF16),
            pltpu.VMEM((n_tp, seq, quarter), BF16),
            pltpu.VMEM((n_tp, seq, head), BF16),
            pltpu.VMEM((seq, head), BF16),
            pltpu.VMEM((1, quarter), F32),
            pltpu.VMEM((n_tp, 1, quarter), F32),
            pltpu.VMEM((n_ep, 1, 128), F32),
            pltpu.VMEM((n_ep, 1, 128), F32),
            pltpu.VMEM((seq, quarter), BF16),
            pltpu.VMEM((2, n_all // 2, seq, quarter), BF16),
            pltpu.VMEM((seq, head), F32),
            pltpu.VMEM((n_tp // 2, n_ep, seq, quarter), BF16),
            pltpu.VMEM((n_tp // 2, n_ep, seq, quarter), BF16),
            pltpu.VMEM((n_tp // 2, n_ep, seq, quarter), BF16),
            pltpu.VMEM((n_all // 2, seq, quarter), BF16),
            pltpu.SemaphoreType.DMA((24,)),
            pltpu.SemaphoreType.DMA((6,)),
            pltpu.SemaphoreType.DMA((6,)),
            pltpu.SemaphoreType.DMA((9,)),
            pltpu.SemaphoreType.DMA((9,)),
            pltpu.SemaphoreType.REGULAR((n_ep.bit_length() - 1,)),
        ],
        compiler_params=pltpu.CompilerParams(
            collective_id=0, has_side_effects=True, vmem_limit_bytes=60 * 1024 * 1024
        ),
    )(*small, *large)


def solution(mesh):
    return jax.shard_map(
        functools.partial(local, mesh.shape["ep"], mesh.shape["tp"]),
        mesh=mesh,
        in_specs=(
            P("ep", "tp"),
            P(),
            P(None, "tp"),
            P(None, "tp"),
            P(None, "tp"),
            P(None, "tp"),
            P(None, "tp"),
            P(None, "tp"),
            P(None, "tp"),
            P("ep", "tp", None, None),
            P("ep", "tp", None),
            P("ep", "tp"),
            P(),
            P("ep", None),
            P("ep", None),
            P("ep", None, "tp"),
            P("ep", None, "tp"),
            P("ep", "tp", None),
            P("tp", "ep"),
            P("tp", "ep"),
            P("ep", "tp"),
            P("tp"),
        ),
        out_specs=P("ep", "tp"),
        check_vma=False,
    )
```

```python
import functools

import jax
import jax.numpy as jnp
from jax import lax
from jax.experimental import pallas as pl
from jax.experimental.pallas import tpu as pltpu
from jax.sharding import PartitionSpec as P

F32 = jnp.float32
BF16 = jnp.bfloat16
MESH = pl.DeviceIdType.MESH
EPS = 1e-06


def dot(a, b):
    return jnp.dot(a, b, preferred_element_type=F32)


def dot_t(a, b):
    return lax.dot_general(a, b, (((1,), (1,)), ((), ())), preferred_element_type=F32)


def column(row):
    n = row.shape[1]
    square = (n, n)
    eye = lax.broadcasted_iota(jnp.int32, square, 0) == lax.broadcasted_iota(jnp.int32, square, 1)
    return jnp.sum(jnp.where(eye, jnp.broadcast_to(row, square), 0.0), axis=1, keepdims=True)


def kernel(
    n_ep,
    n_tp,
    tokens,
    gain_mix,
    w_ig,
    w_fg,
    norm_state,
    max_state,
    gain_ffn,
    ids,
    logits,
    dense_mix,
    w_q,
    w_k,
    w_v,
    w_o,
    w_mix,
    cell,
    e_gate,
    e_up,
    e_down,
    d_gate,
    d_up,
    d_down,
    out,
    tok,
    gm,
    ig_w,
    fg_w,
    ns,
    ms,
    gf,
    id_v,
    lg,
    dmx,
    wp,
    wm,
    cs,
    egu,
    ed,
    dg,
    du,
    dd,
    dgu,
    pack,
    down_own,
    down_far,
    down,
    tok_all,
    mix_all,
    mix_own,
    dm_own,
    dm_all,
    rw_own,
    rw_all,
    res_own,
    res_all,
    read,
    give,
    take,
    c_out,
    c_in,
    local_sem,
    send_sem,
    recv_sem,
    bulk_send,
    bulk_recv,
    word_sem,
):
    i = lax.axis_index("ep")
    j = lax.axis_index("tp")
    seq, quarter = tok.shape
    head = cs.shape[-1]
    ff = e_gate.shape[1]
    lead = ff // 256 * 256
    tail = -(-(ff - lead) // 128) * 128
    half = n_tp // 2
    n_half = n_ep * half
    rows_all = n_ep * seq
    core = lax.rem(j, 2)
    other = 1 - core
    mine = i * half + j // 2
    near = j + 1 - 2 * core
    far = lax.rem(j + 2, n_tp)
    peers = [(i, lax.rem(j + step, n_tp)) for step in range(1, n_tp)]

    cross = lax.rem(near + 2, n_tp)
    span = n_ep // 4
    place = i // span
    group = place // 2

    barrier = pltpu.get_barrier_semaphore()
    bits = [1 << k for k in reversed(range(n_ep.bit_length() - 3))]
    flips = [i + b - 2 * b * lax.rem(i // b, 2) for b in bits]
    lines = jnp.where(place > 0, 1, 0) + jnp.where(place < 3, 1, 0)

    def signal(sem, peer):
        pl.semaphore_signal(sem, inc=1, device_id=peer, device_id_type=MESH)

    def along_line(sem):
        @pl.when(place > 0)
        def _():
            signal(sem, (i - span, j))

        @pl.when(place < 3)
        def _():
            signal(sem, (i + span, j))

    for peer in peers:
        signal(barrier, peer)

    @pl.when(core == 1)
    def _():
        along_line(barrier)
        for f in flips:
            signal(barrier, (f, j))

    local = []

    def fetch(src, dst):
        copy = pltpu.make_async_copy(src, dst, local_sem.at[len(local)])
        copy.start()
        local.append(copy)
        return copy

    got_tok = fetch(tokens, tok)
    got_route = [fetch(ids, id_v), fetch(logits, lg), fetch(dense_mix, dmx)]
    got_dense = [fetch(d_gate, dg), fetch(d_up, du)]
    got_norm = [fetch(gain_mix, gm), fetch(w_ig, ig_w), fetch(w_fg, fg_w)]
    got_proj = [
        fetch(w, wp.at[:, pl.ds(k * head, head)]) for k, w in enumerate((w_q, w_k, w_v, w_o))
    ]
    got_cell = [fetch(cell, cs), fetch(norm_state, ns), fetch(max_state, ms)]
    got_mix = fetch(w_mix, wm)
    got_gf = fetch(gain_ffn, gf)
    got_e = []
    for w, first, last in ((e_gate, 0, 2 * lead), (e_up, lead, 2 * lead + tail)):
        if lead:
            got_e.append(fetch(w.at[0, pl.ds(0, lead)], egu.at[pl.ds(first, lead)]))
        if ff > lead:
            rest = ff - lead
            got_e.append(fetch(w.at[0, pl.ds(lead, rest)], egu.at[pl.ds(last, rest)]))
    got_ed = fetch(e_down.at[0], ed)
    got_dd = fetch(d_down, dd)

    def to_tp(src, dst, phase):
        for peer in peers:
            pltpu.make_async_remote_copy(
                src_ref=src,
                dst_ref=dst.at[j],
                send_sem=send_sem.at[phase],
                recv_sem=recv_sem.at[phase],
                device_id=peer,
                device_id_type=MESH,
            ).start()

    def wait_bytes(buf, count, sem):
        view = buf.at[pl.ds(0, count)]
        pltpu.make_async_copy(view, view, sem).wait()

    def bulk(src, dst, peer, k):
        return pltpu.make_async_remote_copy(
            src_ref=src,
            dst_ref=dst,
            send_sem=bulk_send.at[k],
            recv_sem=bulk_recv.at[k],
            device_id=(i, peer),
            device_id_type=MESH,
        )

    top, low = pl.ds(0, quarter // 2), pl.ds(quarter // 2, quarter // 2)
    far_top = bulk(pack.at[top], dgu.at[j, top], far, 0)
    far_low = bulk(pack.at[low], dgu.at[j, low], far, 1)
    near_gu = bulk(dgu.at[j], dgu.at[j], near, 2)
    near_on = bulk(dgu.at[far], dgu.at[far], near, 3)
    near_down = bulk(down_own, down.at[j // 2], near, 4)
    cross_down = bulk(down_far, down.at[j // 2], cross, 5)
    give_on = [bulk(give.at[g], take.at[g], near, 6 + g) for g in range(2)]
    blocks = [pl.ds(g * (n_half // 2), n_half // 2) for g in range(2)]
    res_on = [
        bulk(res_all.at[other, b], res_all.at[other, b], near, 8 + g) for g, b in enumerate(blocks)
    ]

    got_tok.wait()
    pl.semaphore_wait(barrier, len(peers) + core * (lines + len(flips)))
    to_tp(tok, tok_all, 0)

    @pl.when(core == 1)
    def _():
        along_line(word_sem.at[0])

    tok_all[j] = tok[...]
    for copy in got_route:
        copy.wait()
    l0, l1 = lg[0:1, :], lg[1:2, :]
    s0, s1 = jax.nn.sigmoid(l0 - l1), jax.nn.sigmoid(l1 - l0)

    def put_rw(e, carry):
        rw_own[e, :, 0:seq] = jnp.where(id_v[0:1, :] == e, s0, 0.0) + jnp.where(
            id_v[1:2, :] == e, s1, 0.0
        )
        return carry

    rw_own[...] = jnp.zeros_like(rw_own)
    lax.fori_loop(0, n_ep, put_rw, 0, unroll=8)
    rw_all[i] = rw_own[i]
    mix_row = dmx[...].astype(F32)
    mix_row = jnp.concatenate([mix_row[k : k + 1] for k in range(mix_row.shape[0])], axis=1)
    dm_own[...] = mix_row
    dm_all[j] = mix_row
    if tail > ff - lead > 0:
        for first in (2 * lead, 2 * lead + tail):
            blank = pl.ds(first + ff - lead, tail - ff + lead)
            egu[blank, :] = jnp.zeros((tail - ff + lead, egu.shape[1]), egu.dtype)

    to_tp(dm_own, dm_all, 2)
    for copy in got_dense:
        copy.wait()
    dff = dg.shape[1]
    mid = dff // 2
    square = (dff, dff)
    from_row = lax.broadcasted_iota(jnp.int32, square, 0)
    to_col = lax.broadcasted_iota(jnp.int32, square, 1)

    def pick(hit):
        return jnp.where(hit, 1.0, 0.0).astype(BF16)

    def packed(part):
        first = pick((from_row == to_col + part * mid) & (to_col < mid))
        second = pick((from_row == to_col - mid + part * mid) & (to_col >= mid))
        return (dot(dg[...], first) + dot(du[...], second)).astype(BF16)

    pack[...] = packed(1 - j // 2)
    dgu[j] = packed(j // 2)
    far_top.start()
    near_gu.start()
    for copy in got_norm:
        copy.wait()
    wait_bytes(tok_all, n_tp - 1, recv_sem.at[0])
    full = jnp.concatenate([tok_all[k] for k in range(n_tp)], axis=1).astype(F32)
    scale = lax.rsqrt(jnp.mean(full * full, axis=-1, keepdims=True) + EPS)
    normed = (full * scale * gm[...]).astype(BF16)
    normed_f = normed.astype(F32)
    ig = jnp.sum(normed_f * ig_w[...].astype(F32), axis=-1, keepdims=True)
    fg = jnp.sum(normed_f * fg_w[...].astype(F32), axis=-1, keepdims=True)

    @pl.when(core == 1)
    def _():
        pl.semaphore_wait(word_sem.at[0], lines)
        signal(word_sem.at[1], (i + 2 * span - 4 * span * group, j))
    for copy in got_proj:
        copy.wait()
    proj = dot(normed, wp[...])
    query = proj[:, :head]
    key = proj[:, head : 2 * head] * head ** (-0.5)
    value = proj[:, 2 * head : 3 * head]
    out_gate = proj[:, 3 * head :]
    for copy in got_cell:
        copy.wait()
    carried = jnp.minimum(fg, 0.0) - jnp.log1p(jnp.exp(-jnp.abs(fg))) + column(ms[...])
    stab = jnp.maximum(carried, ig)
    w_old = jnp.exp(carried - stab)
    w_new = jnp.exp(ig - stab) * jnp.sum(query * key, axis=-1, keepdims=True)
    query_t = query.T
    for b in range(seq):
        read[b : b + 1, :] = jnp.sum(query_t[:, b : b + 1] * cs[b], axis=0, keepdims=True)
    numer = w_old * read[...] + w_new * value
    denom = w_old * jnp.sum(query * ns[...], axis=-1, keepdims=True) + w_new
    cell_out = numer / jnp.maximum(jnp.abs(denom), 1.0)
    mixed = (jax.nn.sigmoid(out_gate) * cell_out).astype(BF16)
    mix_own[...] = mixed
    mix_all[j] = mixed
    to_tp(mix_own, mix_all, 3)
    far_low.start()

    @pl.when(core == 1)
    def _():
        pl.semaphore_wait(word_sem.at[1], 1)
        for k, f in enumerate(flips):
            signal(word_sem.at[2 + k], (f, j))
            pl.semaphore_wait(word_sem.at[2 + k], 1)
        signal(word_sem.at[2 + len(flips)], (i, near))
    got_dd.wait()
    some = (down_own.shape[0], dff)
    to_row = lax.broadcasted_iota(jnp.int32, some, 0)
    from_row = lax.broadcasted_iota(jnp.int32, some, 1)

    def half_rows(part):
        hit = (from_row == to_row + part * mid) & (to_row < mid)
        return dot(pick(hit), dd[...]).astype(BF16)

    down_own[...] = half_rows(j // 2)
    down_far[...] = half_rows(1 - j // 2)
    near_down.start()

    got_mix.wait()
    wait_bytes(mix_all, n_tp - 1, recv_sem.at[3])
    heads = jnp.concatenate([mix_all[k] for k in range(n_tp)], axis=1)
    resid = (tok[...].astype(F32) + dot(heads, wm[...])).astype(BF16)
    res_own[...] = resid

    ring = n_ep // 2

    def across(send):
        def body(t, carry):
            turn = (t + 1) // 2
            turn = lax.rem(ring // 2 + ring + jnp.where(lax.rem(t, 2) == 0, turn, -turn), ring)
            high = lax.rem(i // 2 + turn, ring)
            for down_y in (1, 0):
                row = 2 * high + lax.rem(i + down_y, 2)
                for step in reversed(range(half)):
                    send(row, lax.rem(j // 2 + step, half))
            return carry

        lax.fori_loop(0, ring, body, 0, unroll=ring <= 4)

    def send_res(row, col):
        pltpu.make_async_remote_copy(
            src_ref=res_own,
            dst_ref=res_all.at[core, mine],
            send_sem=send_sem.at[4],
            recv_sem=recv_sem.at[4 + 2 * group],
            device_id=(row, 2 * col + other),
            device_id_type=MESH,
        ).start()

    @pl.when(core == 0)
    def _():
        pl.semaphore_wait(word_sem.at[2 + len(flips)], 1)

    def send_rw(step, carry):
        e = lax.rem(i + step, n_ep)
        pltpu.make_async_remote_copy(
            src_ref=rw_own.at[e],
            dst_ref=rw_all.at[i],
            send_sem=send_sem.at[1],
            recv_sem=recv_sem.at[1 + 6 * group],
            device_id=(e, j),
            device_id_type=MESH,
        ).start()
        return carry

    lax.fori_loop(1, n_ep, send_rw, 0)

    across(send_res)
    far_top.wait_recv()
    far_low.wait_recv()
    near_on.start()
    cross_down.start()
    wait_bytes(dm_all, n_tp - 1, recv_sem.at[2])
    got_gf.wait()
    for copy in got_e:
        copy.wait()
    near_gu.wait_recv()
    got_ed.wait()

    lot = rows_all // 2

    def columns(part, k):
        return pl.ds(pl.multiple_of((2 * k + part) * quarter, quarter), quarter)

    def activated(g, u):
        return (g * jax.nn.sigmoid(g) * u).astype(BF16)

    for g in range(2):
        def normalized(part):
            rows = res_all[part, blocks[g]].reshape(n_ep // 2, half, seq, quarter)
            cut, square, logit = [], 0.0, 0.0
            for k in range(half):
                block = rows[:, k].reshape(lot, quarter).astype(F32)
                square += jnp.sum(block * block, axis=-1, keepdims=True)
                block = (block * gf[:, columns(part, k)]).astype(BF16)
                logit += jnp.sum(block.astype(F32) * dm_all[2 * k + part], axis=-1, keepdims=True)
                cut.append(block)
            return cut, square, logit

        def expert_in(cut, part):
            return sum(dot_t(cut[k], egu[:, columns(part, k)]) for k in range(half))

        def dense_in(cut, part):
            return sum(dot(cut[k], dgu[2 * k + part]) for k in range(half))
        wait_bytes(res_all.at[other], n_half // 2, recv_sem.at[4 + 2 * g])
        res_on[g].start()
        cut_a, square_a, logit_a = normalized(other)
        expert_a = expert_in(cut_a, other)
        if g == 0:
            near_on.wait_recv()
        dense_a = dense_in(cut_a, other)
        res_on[g].wait_recv()
        cut_b, square_b, logit_b = normalized(core)
        scale = lax.rsqrt((square_a + square_b) / (n_tp * quarter) + EPS)
        mix_gate = jax.nn.sigmoid((logit_a + logit_b) * scale)
        mids = (expert_a + expert_in(cut_b, core)) * scale
        rest = ff - lead
        hidden = []
        if lead:
            hidden.append(activated(mids[:, :lead], mids[:, lead : 2 * lead]))
        if rest:
            at = 2 * lead
            hidden.append(activated(mids[:, at : at + rest], mids[:, at + tail : at + tail + rest]))
        hidden = jnp.concatenate(hidden, axis=1)
        for here in range(2):

            @pl.when(group == here)
            def _():
                wait_bytes(rw_all, n_ep // 2 - (here == g), recv_sem.at[1 + 6 * g])

        wide = (n_ep // 2, seq, rw_all.shape[-1])
        to_lane = lax.broadcasted_iota(jnp.int32, wide, 2)
        diag = lax.broadcasted_iota(jnp.int32, wide, 1) == to_lane
        mine_rw = rw_all[pl.ds(g * (n_ep // 2), n_ep // 2)]
        some = jnp.where(diag, jnp.broadcast_to(mine_rw, wide), 0.0)
        some = jnp.sum(some.reshape(lot, -1), axis=-1, keepdims=True)
        def expert_part(part, k):
            return dot(hidden, ed[:, columns(part, k)]) * some

        for k in range(half):
            give[g, k] = expert_part(core, k).astype(BF16).reshape(n_ep // 2, seq, quarter)
        give_on[g].start()
        kept = [expert_part(other, k) for k in range(half)]
        mids = (dense_a + dense_in(cut_b, core)) * scale
        middle = activated(mids[:, :mid], mids[:, mid : 2 * mid])
        if g == 0:
            near_down.wait_recv()
            cross_down.wait_recv()
        for k in range(half):
            kept[k] += dot(middle, down[k, 0:mid]) * mix_gate
        give_on[g].wait_recv()
        for k in range(half):
            total = kept[k] + take[g, k].reshape(lot, quarter).astype(F32)
            c_out[k, pl.ds(g * (n_ep // 2), n_ep // 2)] = total.astype(BF16).reshape(
                n_ep // 2, seq, quarter
            )
        first = jnp.where(group == g, 1, 0)

        def send_back(t, carry):
            high = g * (ring // 2) + lax.rem(i // 2 + first + t, ring // 2)
            for down_y in (1, 0):
                row = 2 * high + lax.rem(i + down_y, 2)
                for step in reversed(range(half)):
                    col = lax.rem(j // 2 + step, half)
                    pltpu.make_async_remote_copy(
                        src_ref=c_out.at[col, row],
                        dst_ref=c_in.at[mine],
                        send_sem=send_sem.at[5],
                        recv_sem=recv_sem.at[5],
                        device_id=(row, 2 * col + other),
                        device_id_type=MESH,
                    ).start()
            return carry

        lax.fori_loop(0, ring // 2, send_back, 0, unroll=ring <= 4)
    wait_bytes(tok_all, n_tp - 1, send_sem.at[0])
    wait_bytes(rw_all, n_ep - 1, send_sem.at[1])
    wait_bytes(dm_all, n_tp - 1, send_sem.at[2])
    wait_bytes(mix_all, n_tp - 1, send_sem.at[3])
    wait_bytes(res_all.at[other], n_half, send_sem.at[4])
    for copy in [far_top, far_low, near_gu, near_on, near_down, cross_down] + give_on + res_on:
        copy.wait_send()
    wait_bytes(c_in, n_half, send_sem.at[5])
    wait_bytes(c_in, n_half, recv_sem.at[5])
    def add(k, total):
        return total + c_in[k].astype(F32)

    total = lax.fori_loop(0, n_half, add, res_own[...].astype(F32), unroll=8)
    out[...] = total.astype(BF16)


def local(
    n_ep,
    n_tp,
    tokens,
    gain_mix,
    w_query,
    w_key,
    w_value,
    w_outgate,
    w_input_gate,
    w_forget_gate,
    w_mix_out,
    cell_state,
    norm_state,
    max_state,
    gain_ffn,
    route_ids,
    route_logits,
    expert_gate,
    expert_up,
    expert_down,
    dense_gate,
    dense_up,
    dense_down,
    dense_mix,
):
    seq, quarter = tokens.shape
    features, head = w_query.shape
    n_all = n_ep * n_tp
    ff = expert_gate.shape[2]
    dff = dense_gate.shape[1]
    dff_rows = -(-dff // 32) * 16
    vmem = pl.BlockSpec(memory_space=pltpu.VMEM)
    tail = -(-(ff % 256) // 128) * 128
    wide = 2 * (ff // 256 * 256 + tail)
    any_space = pl.BlockSpec(memory_space=pl.ANY)
    small = (
        tokens,
        gain_mix.reshape(1, -1),
        w_input_gate.reshape(1, -1),
        w_forget_gate.reshape(1, -1),
        norm_state.reshape(seq, head),
        max_state.T,
        gain_ffn.reshape(1, -1),
        route_ids.T,
        route_logits.T,
        dense_mix.reshape(-1, 128),
    )
    large = (
        w_query,
        w_key,
        w_value,
        w_outgate,
        w_mix_out,
        cell_state.reshape(seq, head, head),
        jnp.swapaxes(expert_gate, 1, 2),
        jnp.swapaxes(expert_up, 1, 2),
        expert_down,
        dense_gate,
        dense_up,
        dense_down,
    )
    return pl.pallas_call(
        functools.partial(kernel, n_ep, n_tp),
        out_shape=pltpu.VMEM((seq, quarter), BF16),
        in_specs=[any_space] * (len(small) + len(large)),
        out_specs=vmem,
        scratch_shapes=[pltpu.VMEM(x.shape, x.dtype) for x in small]
        + [
            pltpu.VMEM((features, 4 * head), BF16),
            pltpu.VMEM(w_mix_out.shape, BF16),
            pltpu.VMEM((seq, head, head), F32),
            pltpu.VMEM((wide, features), BF16),
            pltpu.VMEM((ff, features), BF16),
            pltpu.VMEM((quarter, dff), BF16),
            pltpu.VMEM((quarter, dff), BF16),
            pltpu.VMEM((dff, quarter), BF16),
            pltpu.VMEM((n_tp, quarter, dff), BF16),
            pltpu.VMEM((quarter, dff), BF16),
            pltpu.VMEM((dff_rows, quarter), BF16),
            pltpu.VMEM((dff_rows, quarter), BF16),
            pltpu.VMEM((n_tp // 2, dff_rows, quarter), BF16),
            pltpu.VMEM((n_tp, seq, quarter), BF16),
            pltpu.VMEM((n_tp, seq, head), BF16),
            pltpu.VMEM((seq, head), BF16),
            pltpu.VMEM((1, quarter), F32),
            pltpu.VMEM((n_tp, 1, quarter), F32),
            pltpu.VMEM((n_ep, 1, 128), F32),
            pltpu.VMEM((n_ep, 1, 128), F32),
            pltpu.VMEM((seq, quarter), BF16),
            pltpu.VMEM((2, n_all // 2, seq, quarter), BF16),
            pltpu.VMEM((seq, head), F32),
            pltpu.VMEM((2, n_tp // 2, n_ep // 2, seq, quarter), BF16),
            pltpu.VMEM((2, n_tp // 2, n_ep // 2, seq, quarter), BF16),
            pltpu.VMEM((n_tp // 2, n_ep, seq, quarter), BF16),
            pltpu.VMEM((n_all // 2, seq, quarter), BF16),
            pltpu.SemaphoreType.DMA((24,)),
            pltpu.SemaphoreType.DMA((8,)),
            pltpu.SemaphoreType.DMA((8,)),
            pltpu.SemaphoreType.DMA((10,)),
            pltpu.SemaphoreType.DMA((10,)),
            pltpu.SemaphoreType.REGULAR((n_ep.bit_length(),)),
        ],
        compiler_params=pltpu.CompilerParams(
            collective_id=0, has_side_effects=True, vmem_limit_bytes=60 * 1024 * 1024
        ),
    )(*small, *large)


def solution(mesh):
    return jax.shard_map(
        functools.partial(local, mesh.shape["ep"], mesh.shape["tp"]),
        mesh=mesh,
        in_specs=(
            P("ep", "tp"),
            P(),
            P(None, "tp"),
            P(None, "tp"),
            P(None, "tp"),
            P(None, "tp"),
            P(None, "tp"),
            P(None, "tp"),
            P(None, "tp"),
            P("ep", "tp", None, None),
            P("ep", "tp", None),
            P("ep", "tp"),
            P(),
            P("ep", None),
            P("ep", None),
            P("ep", None, "tp"),
            P("ep", None, "tp"),
            P("ep", "tp", None),
            P("tp", "ep"),
            P("tp", "ep"),
            P("ep", "tp"),
            P("tp"),
        ),
        out_specs=P("ep", "tp"),
        check_vma=False,
    )
```

```python
import functools

import jax
import jax.numpy as jnp
from jax import lax
from jax.experimental import pallas as pl
from jax.experimental.pallas import tpu as pltpu
from jax.sharding import PartitionSpec as P

F32 = jnp.float32
BF16 = jnp.bfloat16
N_LOCAL = 6
MESH = pl.DeviceIdType.MESH
EPS = 1e-06


def dot(a, b):
    return jnp.dot(a, b, preferred_element_type=F32)


def dot_t(a, b):
    return lax.dot_general(a, b, (((1,), (1,)), ((), ())), preferred_element_type=F32)


def column(row):
    n = row.shape[1]
    square = (n, n)
    eye = lax.broadcasted_iota(jnp.int32, square, 0) == lax.broadcasted_iota(jnp.int32, square, 1)
    return jnp.sum(jnp.where(eye, jnp.broadcast_to(row, square), 0.0), axis=1, keepdims=True)


def kernel(
    n_ep,
    n_tp,
    tokens,
    gain_mix,
    w_ig,
    w_fg,
    norm_state,
    max_state,
    gain_ffn,
    ids,
    logits,
    dense_mix,
    w_q,
    w_k,
    w_v,
    w_o,
    w_mix,
    cell,
    e_gate,
    e_up,
    e_down,
    d_gate,
    d_up,
    d_down,
    out,
    tok,
    gm,
    ig_w,
    fg_w,
    ns,
    ms,
    gf,
    id_v,
    lg,
    dmx,
    wp,
    wm,
    cs,
    egu,
    turned,
    ed,
    dg,
    du,
    dd,
    dgu,
    pack,
    down_own,
    down_far,
    down,
    tok_all,
    mix_all,
    mix_own,
    dm_own,
    dm_all,
    rw_own,
    rw_all,
    res_own,
    res_all,
    read,
    give,
    take,
    c_out,
    c_in,
    local_sem,
    send_sem,
    recv_sem,
    bulk_send,
    bulk_recv,
    word_sem,
):
    i = lax.axis_index("ep")
    j = lax.axis_index("tp")
    seq, quarter = tok.shape
    head = cs.shape[-1]
    ff = e_gate.shape[1]
    lead = ff // 256 * 256
    tail = -(-(ff - lead) // 128) * 128
    half = n_tp // 2
    n_half = n_ep * half
    rows_all = n_ep * seq
    core = lax.rem(j, 2)
    other = 1 - core
    mine = i * half + j // 2
    near = j + 1 - 2 * core
    far = lax.rem(j + 2, n_tp)
    peers = [(i, lax.rem(j + step, n_tp)) for step in range(1, n_tp)]

    cross = lax.rem(near + 2, n_tp)
    span = n_ep // 4
    place = i // span
    group = place // 2

    barrier = pltpu.get_barrier_semaphore()
    bits = [1 << k for k in reversed(range(n_ep.bit_length() - 3))]
    flips = [i + b - 2 * b * lax.rem(i // b, 2) for b in bits]
    lines = jnp.where(place > 0, 1, 0) + jnp.where(place < 3, 1, 0)

    def signal(sem, peer):
        pl.semaphore_signal(sem, inc=1, device_id=peer, device_id_type=MESH)

    def along_line(sem):
        @pl.when(place > 0)
        def _():
            signal(sem, (i - span, j))

        @pl.when(place < 3)
        def _():
            signal(sem, (i + span, j))

    for peer in peers:
        signal(barrier, peer)

    @pl.when(core == 1)
    def _():
        along_line(barrier)
        for f in flips:
            signal(barrier, (f, j))

    def fetch(src, dst, lot):
        copy = pltpu.make_async_copy(src, dst, local_sem.at[lot])
        copy.start()
        return copy

    got_tok = fetch(tokens, tok, 0)
    got_route = [fetch(*p, 1) for p in ((ids, id_v), (logits, lg), (dense_mix, dmx))]
    got_dense = [fetch(d_gate, dg, 2), fetch(d_up, du, 2)]
    norm_in = ((gain_mix, gm), (w_ig, ig_w), (w_fg, fg_w), (norm_state, ns), (max_state, ms))
    got_norm = [fetch(*p, 3) for p in norm_in]
    got_proj = [
        fetch(w, wp.at[:, pl.ds(k * head, head)], 4) for k, w in enumerate((w_q, w_k, w_v, w_o))
    ]
    got_proj.append(fetch(cell, cs, 4))
    got_late = [fetch(w_mix, wm, 5), fetch(gain_ffn, gf, 5)]
    for w, first, last in ((e_gate, 0, 2 * lead), (e_up, lead, 2 * lead + tail)):
        if lead:
            got_late.append(fetch(w.at[0, pl.ds(0, lead)], egu.at[pl.ds(first, lead)], 5))
        if ff > lead:
            rest = ff - lead
            piece = w.at[0, pl.ds(lead, rest)]
            got_late.append(fetch(piece, egu.at[pl.ds(last, rest)], 5))
    got_late += [fetch(e_down.at[0], ed, 5), fetch(d_down, dd, 5)]

    def to_tp(src, dst, phase):
        for peer in peers:
            pltpu.make_async_remote_copy(
                src_ref=src,
                dst_ref=dst.at[j],
                send_sem=send_sem.at[phase],
                recv_sem=recv_sem.at[phase],
                device_id=peer,
                device_id_type=MESH,
            ).start()

    def wait_bytes(buf, count, sem):
        view = buf.at[pl.ds(0, count)]
        pltpu.make_async_copy(view, view, sem).wait()

    def bulk(src, dst, peer, k):
        return pltpu.make_async_remote_copy(
            src_ref=src,
            dst_ref=dst,
            send_sem=bulk_send.at[k],
            recv_sem=bulk_recv.at[k],
            device_id=(i, peer),
            device_id_type=MESH,
        )

    top, low = pl.ds(0, quarter // 2), pl.ds(quarter // 2, quarter // 2)
    far_top = bulk(pack.at[top], dgu.at[j, top], far, 0)
    far_low = bulk(pack.at[low], dgu.at[j, low], far, 0)
    near_gu = bulk(dgu.at[j], dgu.at[j], near, 1)
    near_on = bulk(dgu.at[far], dgu.at[far], near, 2)
    near_down = bulk(down_own, down.at[j // 2], near, 3)
    cross_down = bulk(down_far, down.at[j // 2], cross, 4)
    give_on = [bulk(give.at[g], take.at[g], near, 5 + g) for g in range(2)]
    blocks = [pl.ds(g * (n_half // 2), n_half // 2) for g in range(2)]
    res_on = [
        bulk(res_all.at[other, b], res_all.at[other, b], near, 7 + g) for g, b in enumerate(blocks)
    ]

    got_tok.wait()
    pl.semaphore_wait(barrier, len(peers) + core * (lines + len(flips)))
    to_tp(tok, tok_all, 0)

    @pl.when(core == 1)
    def _():
        along_line(word_sem.at[0])

    tok_all[j] = tok[...]
    for copy in got_route:
        copy.wait()
    l0, l1 = lg[0:1, :], lg[1:2, :]
    s0, s1 = jax.nn.sigmoid(l0 - l1), jax.nn.sigmoid(l1 - l0)

    def put_rw(e, carry):
        rw_own[e, :, 0:seq] = jnp.where(id_v[0:1, :] == e, s0, 0.0) + jnp.where(
            id_v[1:2, :] == e, s1, 0.0
        )
        return carry

    rw_own[...] = jnp.zeros_like(rw_own)
    lax.fori_loop(0, n_ep, put_rw, 0, unroll=8)
    rw_all[i] = rw_own[i]
    mix_row = dmx[...].astype(F32)
    mix_row = jnp.concatenate([mix_row[k : k + 1] for k in range(mix_row.shape[0])], axis=1)
    dm_own[...] = mix_row
    dm_all[j] = mix_row
    if tail > ff - lead > 0:
        for first in (2 * lead, 2 * lead + tail):
            blank = pl.ds(first + ff - lead, tail - ff + lead)
            egu[blank, :] = jnp.zeros((tail - ff + lead, egu.shape[1]), egu.dtype)

    to_tp(dm_own, dm_all, 2)
    for copy in got_dense:
        copy.wait()
    dff = dg.shape[1]
    mid = dff // 2
    square = (dff, dff)
    from_row = lax.broadcasted_iota(jnp.int32, square, 0)
    to_col = lax.broadcasted_iota(jnp.int32, square, 1)

    def pick(hit):
        return jnp.where(hit, 1.0, 0.0).astype(BF16)

    def packed(part):
        first = pick((from_row == to_col + part * mid) & (to_col < mid))
        second = pick((from_row == to_col - mid + part * mid) & (to_col >= mid))
        return (dot(dg[...], first) + dot(du[...], second)).astype(BF16)

    pack[...] = packed(1 - j // 2)
    dgu[j] = packed(j // 2)
    far_top.start()
    near_gu.start()
    for copy in got_norm:
        copy.wait()
    @pl.when(core == 1)
    def _():
        pl.semaphore_wait(word_sem.at[0], lines)
        signal(word_sem.at[1], (i + 2 * span - 4 * span * group, j))
    wait_bytes(tok_all, n_tp - 1, recv_sem.at[0])
    full = jnp.concatenate([tok_all[k] for k in range(n_tp)], axis=1).astype(F32)
    scale = lax.rsqrt(jnp.mean(full * full, axis=-1, keepdims=True) + EPS)
    normed = (full * scale * gm[...]).astype(BF16)
    normed_f = normed.astype(F32)
    ig = jnp.sum(normed_f * ig_w[...].astype(F32), axis=-1, keepdims=True)
    fg = jnp.sum(normed_f * fg_w[...].astype(F32), axis=-1, keepdims=True)
    carried = jnp.minimum(fg, 0.0) - jnp.log1p(jnp.exp(-jnp.abs(fg))) + column(ms[...])
    stab = jnp.maximum(carried, ig)
    w_old = jnp.exp(carried - stab)
    rise = jnp.exp(ig - stab)
    for copy in got_proj:
        copy.wait()
    proj = dot(normed, wp[...])
    query = proj[:, :head]
    key = proj[:, head : 2 * head] * head ** (-0.5)
    value = proj[:, 2 * head : 3 * head]
    out_gate = proj[:, 3 * head :]
    w_new = rise * jnp.sum(query * key, axis=-1, keepdims=True)
    query_t = query.T
    for b in range(seq):
        read[b : b + 1, :] = jnp.sum(query_t[:, b : b + 1] * cs[b], axis=0, keepdims=True)
    numer = w_old * read[...] + w_new * value
    denom = w_old * jnp.sum(query * ns[...], axis=-1, keepdims=True) + w_new
    cell_out = numer / jnp.maximum(jnp.abs(denom), 1.0)
    mixed = (jax.nn.sigmoid(out_gate) * cell_out).astype(BF16)
    mix_own[...] = mixed
    mix_all[j] = mixed
    to_tp(mix_own, mix_all, 3)
    far_low.start()

    @pl.when(core == 1)
    def _():
        pl.semaphore_wait(word_sem.at[1], 1)
        for k, f in enumerate(flips):
            signal(word_sem.at[2 + k], (f, j))
            pl.semaphore_wait(word_sem.at[2 + k], 1)
        signal(word_sem.at[2 + len(flips)], (i, near))
    for copy in got_late:
        copy.wait()
    some = (down_own.shape[0], dff)
    to_row = lax.broadcasted_iota(jnp.int32, some, 0)
    from_row = lax.broadcasted_iota(jnp.int32, some, 1)

    def half_rows(part):
        hit = (from_row == to_row + part * mid) & (to_row < mid)
        return dot(pick(hit), dd[...]).astype(BF16)

    down_own[...] = half_rows(j // 2)
    down_far[...] = half_rows(1 - j // 2)
    near_down.start()
    wait_bytes(mix_all, n_tp - 1, recv_sem.at[3])
    heads = jnp.concatenate([mix_all[k] for k in range(n_tp)], axis=1)
    resid = (tok[...].astype(F32) + dot(heads, wm[...])).astype(BF16)
    res_own[...] = resid

    ring = n_ep // 2

    def across(send):
        def body(t, carry):
            turn = (t + 1) // 2
            turn = lax.rem(ring // 2 + ring + jnp.where(lax.rem(t, 2) == 0, turn, -turn), ring)
            high = lax.rem(i // 2 + turn, ring)
            for down_y in (1, 0):
                row = 2 * high + lax.rem(i + down_y, 2)
                for step in reversed(range(half)):
                    send(row, lax.rem(j // 2 + step, half))
            return carry

        lax.fori_loop(0, ring, body, 0, unroll=ring <= 4)

    def send_res(row, col):
        pltpu.make_async_remote_copy(
            src_ref=res_own,
            dst_ref=res_all.at[core, mine],
            send_sem=send_sem.at[4],
            recv_sem=recv_sem.at[4 + 2 * group],
            device_id=(row, 2 * col + other),
            device_id_type=MESH,
        ).start()

    @pl.when(core == 0)
    def _():
        pl.semaphore_wait(word_sem.at[2 + len(flips)], 1)

    def send_rw(step, carry):
        e = lax.rem(i + step, n_ep)
        pltpu.make_async_remote_copy(
            src_ref=rw_own.at[e],
            dst_ref=rw_all.at[i],
            send_sem=send_sem.at[1],
            recv_sem=recv_sem.at[1 + 6 * group],
            device_id=(e, j),
            device_id_type=MESH,
        ).start()
        return carry

    lax.fori_loop(1, n_ep, send_rw, 0)

    across(send_res)
    pltpu.make_async_copy(dgu.at[far], dgu.at[far], bulk_recv.at[0]).wait()
    near_on.start()
    wait_bytes(dm_all, n_tp - 1, recv_sem.at[2])
    tile = (quarter, quarter)
    same = lax.broadcasted_iota(jnp.int32, tile, 0) == lax.broadcasted_iota(jnp.int32, tile, 1)
    same = pick(same)
    for q in range(n_tp):
        turned[q] = dot_t(same, egu[:, q * quarter : (q + 1) * quarter]).astype(BF16)
    cross_down.start()
    near_gu.wait_recv()

    lot = rows_all // 2

    def columns(part, k):
        return pl.ds(pl.multiple_of((2 * k + part) * quarter, quarter), quarter)

    def activated(g, u):
        return (g * jax.nn.sigmoid(g) * u).astype(BF16)

    def arrived(g):
        wait_bytes(res_all.at[other], n_half // 2, recv_sem.at[4 + 2 * g])
        res_on[g].start()

    for g in range(2):
        def normalized(part):
            rows = res_all[part, blocks[g]].reshape(n_ep // 2, half, seq, quarter)
            cut, square, logit = [], 0.0, 0.0
            for k in range(half):
                block = rows[:, k].reshape(lot, quarter).astype(F32)
                square += jnp.sum(block * block, axis=-1, keepdims=True)
                block = (block * gf[:, columns(part, k)]).astype(BF16)
                logit += jnp.sum(block.astype(F32) * dm_all[2 * k + part], axis=-1, keepdims=True)
                cut.append(block)
            return cut, square, logit

        def expert_in(cut, part):
            return sum(dot(cut[k], turned[2 * k + part]) for k in range(half))

        def dense_in(cut, part):
            return sum(dot(cut[k], dgu[2 * k + part]) for k in range(half))
        if g == 0:
            arrived(0)
        cut_a, square_a, logit_a = normalized(other)
        expert_a = expert_in(cut_a, other)
        if g == 0:
            near_on.wait_recv()
        dense_a = dense_in(cut_a, other)
        for here in range(2):

            @pl.when(group == here)
            def _():
                wait_bytes(rw_all, n_ep // 2 - (here == g), recv_sem.at[1 + 6 * g])

        wide = (n_ep // 2, seq, rw_all.shape[-1])
        to_lane = lax.broadcasted_iota(jnp.int32, wide, 2)
        diag = lax.broadcasted_iota(jnp.int32, wide, 1) == to_lane
        mine_rw = rw_all[pl.ds(g * (n_ep // 2), n_ep // 2)]
        some = jnp.where(diag, jnp.broadcast_to(mine_rw, wide), 0.0)
        some = jnp.sum(some.reshape(lot, -1), axis=-1, keepdims=True)
        res_on[g].wait_recv()
        cut_b, square_b, logit_b = normalized(core)
        scale = lax.rsqrt((square_a + square_b) / (n_tp * quarter) + EPS)
        mix_gate = jax.nn.sigmoid((logit_a + logit_b) * scale)
        mids = (expert_a + expert_in(cut_b, core)) * scale
        rest = ff - lead
        hidden = []
        if lead:
            hidden.append(activated(mids[:, :lead], mids[:, lead : 2 * lead]))
        if rest:
            at = 2 * lead
            hidden.append(activated(mids[:, at : at + rest], mids[:, at + tail : at + tail + rest]))
        hidden = jnp.concatenate(hidden, axis=1)
        def expert_part(part, k):
            return dot(hidden, ed[:, columns(part, k)]) * some

        for k in range(half):
            give[g, k] = expert_part(core, k).astype(BF16).reshape(n_ep // 2, seq, quarter)
        give_on[g].start()
        kept = [expert_part(other, k) for k in range(half)]
        if g == 0:
            arrived(1)
        mids = (dense_a + dense_in(cut_b, core)) * scale
        middle = activated(mids[:, :mid], mids[:, mid : 2 * mid])
        if g == 0:
            near_down.wait_recv()
            cross_down.wait_recv()
        for k in range(half):
            kept[k] += dot(middle, down[k, 0:mid]) * mix_gate
        give_on[g].wait_recv()
        for k in range(half):
            total = kept[k] + take[g, k].reshape(lot, quarter).astype(F32)
            c_out[k, pl.ds(g * (n_ep // 2), n_ep // 2)] = total.astype(BF16).reshape(
                n_ep // 2, seq, quarter
            )
        first = jnp.where(group == g, 1, 0)

        def send_back(t, carry):
            high = g * (ring // 2) + lax.rem(i // 2 + first + t, ring // 2)
            for down_y in (1, 0):
                row = 2 * high + lax.rem(i + down_y, 2)
                for step in reversed(range(half)):
                    col = lax.rem(j // 2 + step, half)
                    pltpu.make_async_remote_copy(
                        src_ref=c_out.at[col, row],
                        dst_ref=c_in.at[mine],
                        send_sem=send_sem.at[5],
                        recv_sem=recv_sem.at[5],
                        device_id=(row, 2 * col + other),
                        device_id_type=MESH,
                    ).start()
            return carry

        lax.fori_loop(0, ring // 2, send_back, 0, unroll=ring <= 4)
    wait_bytes(tok_all, n_tp - 1, send_sem.at[0])
    wait_bytes(rw_all, n_ep - 1, send_sem.at[1])
    wait_bytes(dm_all, n_tp - 1, send_sem.at[2])
    wait_bytes(mix_all, n_tp - 1, send_sem.at[3])
    wait_bytes(res_all.at[other], n_half, send_sem.at[4])
    pltpu.make_async_copy(pack, pack, bulk_send.at[0]).wait()
    for copy in [near_gu, near_on, near_down, cross_down] + give_on + res_on:
        copy.wait_send()
    wait_bytes(c_in, n_half, send_sem.at[5])
    wait_bytes(c_in, n_half, recv_sem.at[5])
    def add(k, total):
        return total + c_in[k].astype(F32)

    total = lax.fori_loop(0, n_half, add, res_own[...].astype(F32), unroll=8)
    out[...] = total.astype(BF16)


def local(
    n_ep,
    n_tp,
    tokens,
    gain_mix,
    w_query,
    w_key,
    w_value,
    w_outgate,
    w_input_gate,
    w_forget_gate,
    w_mix_out,
    cell_state,
    norm_state,
    max_state,
    gain_ffn,
    route_ids,
    route_logits,
    expert_gate,
    expert_up,
    expert_down,
    dense_gate,
    dense_up,
    dense_down,
    dense_mix,
):
    seq, quarter = tokens.shape
    features, head = w_query.shape
    n_all = n_ep * n_tp
    ff = expert_gate.shape[2]
    dff = dense_gate.shape[1]
    dff_rows = -(-dff // 32) * 16
    vmem = pl.BlockSpec(memory_space=pltpu.VMEM)
    tail = -(-(ff % 256) // 128) * 128
    wide = 2 * (ff // 256 * 256 + tail)
    any_space = pl.BlockSpec(memory_space=pl.ANY)
    small = (
        tokens,
        gain_mix.reshape(1, -1),
        w_input_gate.reshape(1, -1),
        w_forget_gate.reshape(1, -1),
        norm_state.reshape(seq, head),
        max_state.T,
        gain_ffn.reshape(1, -1),
        route_ids.T,
        route_logits.T,
        dense_mix.reshape(-1, 128),
    )
    large = (
        w_query,
        w_key,
        w_value,
        w_outgate,
        w_mix_out,
        cell_state.reshape(seq, head, head),
        jnp.swapaxes(expert_gate, 1, 2),
        jnp.swapaxes(expert_up, 1, 2),
        expert_down,
        dense_gate,
        dense_up,
        dense_down,
    )
    return pl.pallas_call(
        functools.partial(kernel, n_ep, n_tp),
        out_shape=pltpu.VMEM((seq, quarter), BF16),
        in_specs=[any_space] * (len(small) + len(large)),
        out_specs=vmem,
        scratch_shapes=[pltpu.VMEM(x.shape, x.dtype) for x in small]
        + [
            pltpu.VMEM((features, 4 * head), BF16),
            pltpu.VMEM(w_mix_out.shape, BF16),
            pltpu.VMEM((seq, head, head), F32),
            pltpu.VMEM((wide, features), BF16),
            pltpu.VMEM((n_tp, quarter, wide), BF16),
            pltpu.VMEM((ff, features), BF16),
            pltpu.VMEM((quarter, dff), BF16),
            pltpu.VMEM((quarter, dff), BF16),
            pltpu.VMEM((dff, quarter), BF16),
            pltpu.VMEM((n_tp, quarter, dff), BF16),
            pltpu.VMEM((quarter, dff), BF16),
            pltpu.VMEM((dff_rows, quarter), BF16),
            pltpu.VMEM((dff_rows, quarter), BF16),
            pltpu.VMEM((n_tp // 2, dff_rows, quarter), BF16),
            pltpu.VMEM((n_tp, seq, quarter), BF16),
            pltpu.VMEM((n_tp, seq, head), BF16),
            pltpu.VMEM((seq, head), BF16),
            pltpu.VMEM((1, quarter), F32),
            pltpu.VMEM((n_tp, 1, quarter), F32),
            pltpu.VMEM((n_ep, 1, 128), F32),
            pltpu.VMEM((n_ep, 1, 128), F32),
            pltpu.VMEM((seq, quarter), BF16),
            pltpu.VMEM((2, n_all // 2, seq, quarter), BF16),
            pltpu.VMEM((seq, head), F32),
            pltpu.VMEM((2, n_tp // 2, n_ep // 2, seq, quarter), BF16),
            pltpu.VMEM((2, n_tp // 2, n_ep // 2, seq, quarter), BF16),
            pltpu.VMEM((n_tp // 2, n_ep, seq, quarter), BF16),
            pltpu.VMEM((n_all // 2, seq, quarter), BF16),
            pltpu.SemaphoreType.DMA((N_LOCAL,)),
            pltpu.SemaphoreType.DMA((6,)),
            pltpu.SemaphoreType.DMA((8,)),
            pltpu.SemaphoreType.DMA((9,)),
            pltpu.SemaphoreType.DMA((9,)),
            pltpu.SemaphoreType.REGULAR((n_ep.bit_length(),)),
        ],
        compiler_params=pltpu.CompilerParams(
            collective_id=0, has_side_effects=True, vmem_limit_bytes=60 * 1024 * 1024
        ),
    )(*small, *large)


def solution(mesh):
    return jax.shard_map(
        functools.partial(local, mesh.shape["ep"], mesh.shape["tp"]),
        mesh=mesh,
        in_specs=(
            P("ep", "tp"),
            P(),
            P(None, "tp"),
            P(None, "tp"),
            P(None, "tp"),
            P(None, "tp"),
            P(None, "tp"),
            P(None, "tp"),
            P(None, "tp"),
            P("ep", "tp", None, None),
            P("ep", "tp", None),
            P("ep", "tp"),
            P(),
            P("ep", None),
            P("ep", None),
            P("ep", None, "tp"),
            P("ep", None, "tp"),
            P("ep", "tp", None),
            P("tp", "ep"),
            P("tp", "ep"),
            P("ep", "tp"),
            P("tp"),
        ),
        out_specs=P("ep", "tp"),
        check_vma=False,
    )
```

```python
import functools

import jax
import jax.numpy as jnp
from jax import lax
from jax.experimental import pallas as pl
from jax.experimental.pallas import tpu as pltpu
from jax.sharding import PartitionSpec as P

F32 = jnp.float32
BF16 = jnp.bfloat16
N_LOCAL = 6
MESH = pl.DeviceIdType.MESH
EPS = 1e-06


def dot(a, b):
    return jnp.dot(a, b, preferred_element_type=F32)


def dot_t(a, b):
    return lax.dot_general(a, b, (((1,), (1,)), ((), ())), preferred_element_type=F32)


def column(row):
    n = row.shape[1]
    square = (n, n)
    eye = lax.broadcasted_iota(jnp.int32, square, 0) == lax.broadcasted_iota(jnp.int32, square, 1)
    return jnp.sum(jnp.where(eye, jnp.broadcast_to(row, square), 0.0), axis=1, keepdims=True)


def kernel(
    n_ep,
    n_tp,
    tokens,
    gain_mix,
    w_ig,
    w_fg,
    norm_state,
    max_state,
    gain_ffn,
    ids,
    logits,
    dense_mix,
    w_q,
    w_k,
    w_v,
    w_o,
    w_mix,
    cell,
    e_gate,
    e_up,
    e_down,
    d_gate,
    d_up,
    d_down,
    out,
    tok,
    gm,
    ig_w,
    fg_w,
    ns,
    ms,
    gf,
    id_v,
    lg,
    dmx,
    wp,
    wm,
    cs,
    egu,
    turned,
    ed,
    dg,
    du,
    dd,
    dgu,
    pack,
    down_own,
    down_far,
    down,
    tok_all,
    mix_all,
    mix_own,
    dm_own,
    dm_all,
    rw_own,
    rw_all,
    res_own,
    res_all,
    read,
    give_a,
    give_b,
    take_a,
    take_b,
    c_out,
    c_in,
    local_sem,
    send_sem,
    recv_sem,
    bulk_recv,
    word_sem,
):
    i = lax.axis_index("ep")
    j = lax.axis_index("tp")
    seq, quarter = tok.shape
    head = cs.shape[-1]
    ff = e_gate.shape[1]
    lead = ff // 256 * 256
    tail = -(-(ff - lead) // 128) * 128
    half = n_tp // 2
    n_half = n_ep * half
    rows_all = n_ep * seq
    core = lax.rem(j, 2)
    other = 1 - core
    mine = i * half + j // 2
    near = j + 1 - 2 * core
    far = lax.rem(j + 2, n_tp)
    peers = [(i, lax.rem(j + step, n_tp)) for step in range(1, n_tp)]

    cross = lax.rem(near + 2, n_tp)
    span = n_ep // 4
    place = i // span
    group = jnp.minimum(place, 1)
    edges = (0, span, n_ep)
    counts = (span, n_ep - span)

    barrier = pltpu.get_barrier_semaphore()
    bits = [1 << k for k in reversed(range(n_ep.bit_length() - 3))]
    flips = [i + b - 2 * b * lax.rem(i // b, 2) for b in bits]
    lines = jnp.where(place > 0, 1, 0) + jnp.where(place < 3, 1, 0)

    def signal(sem, peer):
        pl.semaphore_signal(sem, inc=1, device_id=peer, device_id_type=MESH)

    def along_line(sem):
        @pl.when(place > 0)
        def _():
            signal(sem, (i - span, j))

        @pl.when(place < 3)
        def _():
            signal(sem, (i + span, j))

    for peer in peers:
        signal(barrier, peer)

    @pl.when(core == 1)
    def _():
        along_line(barrier)
        for f in flips:
            signal(barrier, (f, j))

    def fetch(src, dst, lot):
        copy = pltpu.make_async_copy(src, dst, local_sem.at[lot])
        copy.start()
        return copy

    got_tok = fetch(tokens, tok, 0)
    got_route = [fetch(*p, 1) for p in ((ids, id_v), (logits, lg), (dense_mix, dmx))]
    got_dense = [fetch(d_gate, dg, 2), fetch(d_up, du, 2)]
    norm_in = ((gain_mix, gm), (w_ig, ig_w), (w_fg, fg_w), (norm_state, ns), (max_state, ms))
    got_norm = [fetch(*p, 3) for p in norm_in]
    got_proj = [
        fetch(w, wp.at[:, pl.ds(k * head, head)], 4) for k, w in enumerate((w_q, w_k, w_v, w_o))
    ]
    got_proj.append(fetch(cell, cs, 4))
    got_late = [fetch(w_mix, wm, 5), fetch(gain_ffn, gf, 5)]
    for w, first, last in ((e_gate, 0, 2 * lead), (e_up, lead, 2 * lead + tail)):
        if lead:
            got_late.append(fetch(w.at[0, pl.ds(0, lead)], egu.at[pl.ds(first, lead)], 5))
        if ff > lead:
            rest = ff - lead
            piece = w.at[0, pl.ds(lead, rest)]
            got_late.append(fetch(piece, egu.at[pl.ds(last, rest)], 5))
    got_late += [fetch(e_down.at[0], ed, 5), fetch(d_down, dd, 5)]

    def to_tp(src, dst, phase):
        for peer in peers:
            pltpu.make_async_remote_copy(
                src_ref=src,
                dst_ref=dst.at[j],
                send_sem=send_sem.at[0],
                recv_sem=recv_sem.at[phase],
                device_id=peer,
                device_id_type=MESH,
            ).start()

    def wait_bytes(buf, count, sem):
        view = buf.at[pl.ds(0, count)]
        pltpu.make_async_copy(view, view, sem).wait()

    def bulk(src, dst, peer, k):
        return pltpu.make_async_remote_copy(
            src_ref=src,
            dst_ref=dst,
            send_sem=send_sem.at[0],
            recv_sem=bulk_recv.at[k],
            device_id=(i, peer),
            device_id_type=MESH,
        )

    top, low = pl.ds(0, quarter // 2), pl.ds(quarter // 2, quarter // 2)
    far_top = bulk(pack.at[top], dgu.at[j, top], far, 0)
    far_low = bulk(pack.at[low], dgu.at[j, low], far, 0)
    near_gu = bulk(dgu.at[j], dgu.at[j], near, 1)
    near_on = bulk(dgu.at[far], dgu.at[far], near, 2)
    near_down = bulk(down_own, down.at[j // 2], near, 3)
    cross_down = bulk(down_far, down.at[j // 2], cross, 4)
    give, take = (give_a, give_b), (take_a, take_b)
    give_on = [bulk(give[g], take[g], near, 5 + g) for g in range(2)]
    blocks = [pl.ds(edges[g] * half, counts[g] * half) for g in range(2)]
    res_on = [
        bulk(res_all.at[other, b], res_all.at[other, b], near, 7 + g) for g, b in enumerate(blocks)
    ]

    got_tok.wait()
    pl.semaphore_wait(barrier, len(peers) + core * (lines + len(flips)))
    to_tp(tok, tok_all, 0)

    @pl.when(core == 1)
    def _():
        along_line(word_sem.at[0])

    tok_all[j] = tok[...]
    for copy in got_route:
        copy.wait()
    l0, l1 = lg[0:1, :], lg[1:2, :]
    s0, s1 = jax.nn.sigmoid(l0 - l1), jax.nn.sigmoid(l1 - l0)

    def put_rw(e, carry):
        rw_own[e, :, 0:seq] = jnp.where(id_v[0:1, :] == e, s0, 0.0) + jnp.where(
            id_v[1:2, :] == e, s1, 0.0
        )
        return carry

    rw_own[...] = jnp.zeros_like(rw_own)
    lax.fori_loop(0, n_ep, put_rw, 0, unroll=8)
    rw_all[i] = rw_own[i]
    mix_row = dmx[...].astype(F32)
    mix_row = jnp.concatenate([mix_row[k : k + 1] for k in range(mix_row.shape[0])], axis=1)
    dm_own[...] = mix_row
    dm_all[j] = mix_row
    if tail > ff - lead > 0:
        for first in (2 * lead, 2 * lead + tail):
            blank = pl.ds(first + ff - lead, tail - ff + lead)
            egu[blank, :] = jnp.zeros((tail - ff + lead, egu.shape[1]), egu.dtype)

    to_tp(dm_own, dm_all, 2)
    for copy in got_dense:
        copy.wait()
    dff = dg.shape[1]
    mid = dff // 2
    square = (dff, dff)
    from_row = lax.broadcasted_iota(jnp.int32, square, 0)
    to_col = lax.broadcasted_iota(jnp.int32, square, 1)

    def pick(hit):
        return jnp.where(hit, 1.0, 0.0).astype(BF16)

    def packed(part):
        first = pick((from_row == to_col + part * mid) & (to_col < mid))
        second = pick((from_row == to_col - mid + part * mid) & (to_col >= mid))
        return (dot(dg[...], first) + dot(du[...], second)).astype(BF16)

    pack[...] = packed(1 - j // 2)
    dgu[j] = packed(j // 2)
    far_top.start()
    near_gu.start()
    for copy in got_norm:
        copy.wait()
    @pl.when(core == 1)
    def _():
        pl.semaphore_wait(word_sem.at[0], lines)
        signal(word_sem.at[1], (i + 2 * span - 4 * span * (place // 2), j))
    wait_bytes(tok_all, n_tp - 1, recv_sem.at[0])
    full = jnp.concatenate([tok_all[k] for k in range(n_tp)], axis=1).astype(F32)
    scale = lax.rsqrt(jnp.mean(full * full, axis=-1, keepdims=True) + EPS)
    normed = (full * scale * gm[...]).astype(BF16)
    normed_f = normed.astype(F32)
    ig = jnp.sum(normed_f * ig_w[...].astype(F32), axis=-1, keepdims=True)
    fg = jnp.sum(normed_f * fg_w[...].astype(F32), axis=-1, keepdims=True)
    carried = jnp.minimum(fg, 0.0) - jnp.log1p(jnp.exp(-jnp.abs(fg))) + column(ms[...])
    stab = jnp.maximum(carried, ig)
    w_old = jnp.exp(carried - stab)
    rise = jnp.exp(ig - stab)
    for copy in got_proj:
        copy.wait()
    proj = dot(normed, wp[...])
    query = proj[:, :head]
    key = proj[:, head : 2 * head] * head ** (-0.5)
    value = proj[:, 2 * head : 3 * head]
    out_gate = proj[:, 3 * head :]
    w_new = rise * jnp.sum(query * key, axis=-1, keepdims=True)
    query_t = query.T
    for b in range(seq):
        read[b : b + 1, :] = jnp.sum(query_t[:, b : b + 1] * cs[b], axis=0, keepdims=True)
    numer = w_old * read[...] + w_new * value
    denom = w_old * jnp.sum(query * ns[...], axis=-1, keepdims=True) + w_new
    cell_out = numer / jnp.maximum(jnp.abs(denom), 1.0)
    mixed = (jax.nn.sigmoid(out_gate) * cell_out).astype(BF16)
    mix_own[...] = mixed
    mix_all[j] = mixed
    to_tp(mix_own, mix_all, 3)
    far_low.start()

    @pl.when(core == 1)
    def _():
        pl.semaphore_wait(word_sem.at[1], 1)
        for k, f in enumerate(flips):
            signal(word_sem.at[2 + k], (f, j))
            pl.semaphore_wait(word_sem.at[2 + k], 1)
        signal(word_sem.at[2 + len(flips)], (i, near))
    for copy in got_late:
        copy.wait()
    some = (down_own.shape[0], dff)
    to_row = lax.broadcasted_iota(jnp.int32, some, 0)
    from_row = lax.broadcasted_iota(jnp.int32, some, 1)

    def half_rows(part):
        hit = (from_row == to_row + part * mid) & (to_row < mid)
        return dot(pick(hit), dd[...]).astype(BF16)

    down_own[...] = half_rows(j // 2)
    down_far[...] = half_rows(1 - j // 2)
    near_down.start()
    wait_bytes(mix_all, n_tp - 1, recv_sem.at[3])
    heads = jnp.concatenate([mix_all[k] for k in range(n_tp)], axis=1)
    resid = (tok[...].astype(F32) + dot(heads, wm[...])).astype(BF16)
    res_own[...] = resid

    ring = n_ep // 2

    def across(send):
        def body(t, carry):
            turn = (t + 1) // 2
            turn = lax.rem(ring // 2 + ring + jnp.where(lax.rem(t, 2) == 0, turn, -turn), ring)
            high = lax.rem(i // 2 + turn, ring)
            for down_y in (1, 0):
                row = 2 * high + lax.rem(i + down_y, 2)
                for step in reversed(range(half)):
                    send(row, lax.rem(j // 2 + step, half))
            return carry

        lax.fori_loop(0, ring, body, 0, unroll=ring <= 4)

    def send_res(row, col):
        pltpu.make_async_remote_copy(
            src_ref=res_own,
            dst_ref=res_all.at[core, mine],
            send_sem=send_sem.at[0],
            recv_sem=recv_sem.at[4 + 2 * group],
            device_id=(row, 2 * col + other),
            device_id_type=MESH,
        ).start()

    @pl.when(core == 0)
    def _():
        pl.semaphore_wait(word_sem.at[2 + len(flips)], 1)

    def send_rw(step, carry):
        e = lax.rem(i + step, n_ep)
        pltpu.make_async_remote_copy(
            src_ref=rw_own.at[e],
            dst_ref=rw_all.at[i],
            send_sem=send_sem.at[0],
            recv_sem=recv_sem.at[1 + 6 * group],
            device_id=(e, j),
            device_id_type=MESH,
        ).start()
        return carry

    lax.fori_loop(1, n_ep, send_rw, 0)

    across(send_res)
    pltpu.make_async_copy(dgu.at[far], dgu.at[far], bulk_recv.at[0]).wait()
    near_on.start()
    wait_bytes(dm_all, n_tp - 1, recv_sem.at[2])
    tile = (quarter, quarter)
    same = lax.broadcasted_iota(jnp.int32, tile, 0) == lax.broadcasted_iota(jnp.int32, tile, 1)
    same = pick(same)
    for q in range(n_tp):
        turned[q] = dot_t(same, egu[:, q * quarter : (q + 1) * quarter]).astype(BF16)
    cross_down.start()
    near_gu.wait_recv()


    def columns(part, k):
        return pl.ds(pl.multiple_of((2 * k + part) * quarter, quarter), quarter)

    def activated(g, u):
        return (g * jax.nn.sigmoid(g) * u).astype(BF16)

    def arrived(g):
        wait_bytes(res_all.at[other], counts[g] * half, recv_sem.at[4 + 2 * g])
        res_on[g].start()

    for g in range(2):
        n_rows = counts[g]
        lot = n_rows * seq

        def normalized(part):
            rows = res_all[part, blocks[g]].reshape(n_rows, half, seq, quarter)
            cut, square, logit = [], 0.0, 0.0
            for k in range(half):
                block = rows[:, k].reshape(lot, quarter).astype(F32)
                square += jnp.sum(block * block, axis=-1, keepdims=True)
                block = (block * gf[:, columns(part, k)]).astype(BF16)
                logit += jnp.sum(block.astype(F32) * dm_all[2 * k + part], axis=-1, keepdims=True)
                cut.append(block)
            return cut, square, logit

        def expert_in(cut, part):
            return sum(dot(cut[k], turned[2 * k + part]) for k in range(half))

        def dense_in(cut, part):
            return sum(dot(cut[k], dgu[2 * k + part]) for k in range(half))
        if g == 0:
            arrived(0)
        cut_a, square_a, logit_a = normalized(other)
        expert_a = expert_in(cut_a, other)
        if g == 0:
            near_on.wait_recv()
        dense_a = dense_in(cut_a, other)
        for here in range(2):

            @pl.when(group == here)
            def _():
                wait_bytes(rw_all, n_rows - (here == g), recv_sem.at[1 + 6 * g])

        wide = (n_rows, seq, rw_all.shape[-1])
        to_lane = lax.broadcasted_iota(jnp.int32, wide, 2)
        diag = lax.broadcasted_iota(jnp.int32, wide, 1) == to_lane
        mine_rw = rw_all[pl.ds(edges[g], n_rows)]
        some = jnp.where(diag, jnp.broadcast_to(mine_rw, wide), 0.0)
        some = jnp.sum(some.reshape(lot, -1), axis=-1, keepdims=True)
        res_on[g].wait_recv()
        cut_b, square_b, logit_b = normalized(core)
        scale = lax.rsqrt((square_a + square_b) / (n_tp * quarter) + EPS)
        mix_gate = jax.nn.sigmoid((logit_a + logit_b) * scale)
        mids = (expert_a + expert_in(cut_b, core)) * scale
        rest = ff - lead
        hidden = []
        if lead:
            hidden.append(activated(mids[:, :lead], mids[:, lead : 2 * lead]))
        if rest:
            at = 2 * lead
            hidden.append(activated(mids[:, at : at + rest], mids[:, at + tail : at + tail + rest]))
        hidden = jnp.concatenate(hidden, axis=1)
        def expert_part(part, k):
            return dot(hidden, ed[:, columns(part, k)]) * some

        for k in range(half):
            give[g][k] = expert_part(core, k).astype(BF16).reshape(n_rows, seq, quarter)
        give_on[g].start()
        kept = [expert_part(other, k) for k in range(half)]
        mids = (dense_a + dense_in(cut_b, core)) * scale
        middle = activated(mids[:, :mid], mids[:, mid : 2 * mid])
        if g == 0:
            near_down.wait_recv()
            cross_down.wait_recv()
        for k in range(half):
            kept[k] += dot(middle, down[k, 0:mid]) * mix_gate
        give_on[g].wait_recv()
        for k in range(half):
            total = kept[k] + take[g][k].reshape(lot, quarter).astype(F32)
            c_out[k, pl.ds(edges[g], n_rows)] = total.astype(BF16).reshape(n_rows, seq, quarter)
        def send_back(row, carry):
            for col in range(half):
                pltpu.make_async_remote_copy(
                    src_ref=c_out.at[col, row],
                    dst_ref=c_in.at[mine],
                    send_sem=send_sem.at[0],
                    recv_sem=recv_sem.at[5],
                    device_id=(row, 2 * col + other),
                    device_id_type=MESH,
                ).start()
            return carry

        lax.fori_loop(edges[g], edges[g + 1], send_back, 0, unroll=n_ep <= 8)
        if g == 0:
            arrived(1)
    wait_bytes(tok_all, n_tp - 1, send_sem.at[0])
    wait_bytes(rw_all, n_ep - 1, send_sem.at[0])
    wait_bytes(dm_all, n_tp - 1, send_sem.at[0])
    wait_bytes(mix_all, n_tp - 1, send_sem.at[0])
    wait_bytes(res_all.at[other], n_half, send_sem.at[0])
    pltpu.make_async_copy(pack, pack, send_sem.at[0]).wait()
    for copy in [near_gu, near_on, near_down, cross_down] + give_on + res_on:
        copy.wait_send()
    wait_bytes(c_in, n_half, send_sem.at[0])
    wait_bytes(c_in, n_half, recv_sem.at[5])
    def add(k, total):
        return total + c_in[k].astype(F32)

    total = lax.fori_loop(0, n_half, add, res_own[...].astype(F32), unroll=8)
    out[...] = total.astype(BF16)


def local(
    n_ep,
    n_tp,
    tokens,
    gain_mix,
    w_query,
    w_key,
    w_value,
    w_outgate,
    w_input_gate,
    w_forget_gate,
    w_mix_out,
    cell_state,
    norm_state,
    max_state,
    gain_ffn,
    route_ids,
    route_logits,
    expert_gate,
    expert_up,
    expert_down,
    dense_gate,
    dense_up,
    dense_down,
    dense_mix,
):
    seq, quarter = tokens.shape
    features, head = w_query.shape
    n_all = n_ep * n_tp
    ff = expert_gate.shape[2]
    dff = dense_gate.shape[1]
    dff_rows = -(-dff // 32) * 16
    vmem = pl.BlockSpec(memory_space=pltpu.VMEM)
    tail = -(-(ff % 256) // 128) * 128
    wide = 2 * (ff // 256 * 256 + tail)
    any_space = pl.BlockSpec(memory_space=pl.ANY)
    small = (
        tokens,
        gain_mix.reshape(1, -1),
        w_input_gate.reshape(1, -1),
        w_forget_gate.reshape(1, -1),
        norm_state.reshape(seq, head),
        max_state.T,
        gain_ffn.reshape(1, -1),
        route_ids.T,
        route_logits.T,
        dense_mix.reshape(-1, 128),
    )
    large = (
        w_query,
        w_key,
        w_value,
        w_outgate,
        w_mix_out,
        cell_state.reshape(seq, head, head),
        jnp.swapaxes(expert_gate, 1, 2),
        jnp.swapaxes(expert_up, 1, 2),
        expert_down,
        dense_gate,
        dense_up,
        dense_down,
    )
    return pl.pallas_call(
        functools.partial(kernel, n_ep, n_tp),
        out_shape=pltpu.VMEM((seq, quarter), BF16),
        in_specs=[any_space] * (len(small) + len(large)),
        out_specs=vmem,
        scratch_shapes=[pltpu.VMEM(x.shape, x.dtype) for x in small]
        + [
            pltpu.VMEM((features, 4 * head), BF16),
            pltpu.VMEM(w_mix_out.shape, BF16),
            pltpu.VMEM((seq, head, head), F32),
            pltpu.VMEM((wide, features), BF16),
            pltpu.VMEM((n_tp, quarter, wide), BF16),
            pltpu.VMEM((ff, features), BF16),
            pltpu.VMEM((quarter, dff), BF16),
            pltpu.VMEM((quarter, dff), BF16),
            pltpu.VMEM((dff, quarter), BF16),
            pltpu.VMEM((n_tp, quarter, dff), BF16),
            pltpu.VMEM((quarter, dff), BF16),
            pltpu.VMEM((dff_rows, quarter), BF16),
            pltpu.VMEM((dff_rows, quarter), BF16),
            pltpu.VMEM((n_tp // 2, dff_rows, quarter), BF16),
            pltpu.VMEM((n_tp, seq, quarter), BF16),
            pltpu.VMEM((n_tp, seq, head), BF16),
            pltpu.VMEM((seq, head), BF16),
            pltpu.VMEM((1, quarter), F32),
            pltpu.VMEM((n_tp, 1, quarter), F32),
            pltpu.VMEM((n_ep, 1, 128), F32),
            pltpu.VMEM((n_ep, 1, 128), F32),
            pltpu.VMEM((seq, quarter), BF16),
            pltpu.VMEM((2, n_all // 2, seq, quarter), BF16),
            pltpu.VMEM((seq, head), F32),
            pltpu.VMEM((n_tp // 2, n_ep // 4, seq, quarter), BF16),
            pltpu.VMEM((n_tp // 2, n_ep - n_ep // 4, seq, quarter), BF16),
            pltpu.VMEM((n_tp // 2, n_ep // 4, seq, quarter), BF16),
            pltpu.VMEM((n_tp // 2, n_ep - n_ep // 4, seq, quarter), BF16),
            pltpu.VMEM((n_tp // 2, n_ep, seq, quarter), BF16),
            pltpu.VMEM((n_all // 2, seq, quarter), BF16),
            pltpu.SemaphoreType.DMA((N_LOCAL,)),
            pltpu.SemaphoreType.DMA((1,)),
            pltpu.SemaphoreType.DMA((8,)),
            pltpu.SemaphoreType.DMA((9,)),
            pltpu.SemaphoreType.REGULAR((n_ep.bit_length(),)),
        ],
        compiler_params=pltpu.CompilerParams(
            collective_id=0, has_side_effects=True, vmem_limit_bytes=60 * 1024 * 1024
        ),
    )(*small, *large)


def solution(mesh):
    return jax.shard_map(
        functools.partial(local, mesh.shape["ep"], mesh.shape["tp"]),
        mesh=mesh,
        in_specs=(
            P("ep", "tp"),
            P(),
            P(None, "tp"),
            P(None, "tp"),
            P(None, "tp"),
            P(None, "tp"),
            P(None, "tp"),
            P(None, "tp"),
            P(None, "tp"),
            P("ep", "tp", None, None),
            P("ep", "tp", None),
            P("ep", "tp"),
            P(),
            P("ep", None),
            P("ep", None),
            P("ep", None, "tp"),
            P("ep", None, "tp"),
            P("ep", "tp", None),
            P("tp", "ep"),
            P("tp", "ep"),
            P("ep", "tp"),
            P("tp"),
        ),
        out_specs=P("ep", "tp"),
        check_vma=False,
    )
```
